256 devices in a mesh: ep: 64 (over z, x, core), tp: 4 (over y).
Axes of the slice: x: 4, y: 4, z: 8, core: 2. Of those that a mesh axis runs over, the one named last changes fastest.
Arguments:
- projected_queries: bfloat16 [16384, 2048], P('ep', 'tp'), may hold values from -245 to 245, as said below
- key_proj: bfloat16 [16384, 512], P('ep', 'tp'), may hold values from -6.2 to 6.2
- projected_values: bfloat16 [16384, 512], P('ep', 'tp'), may hold values from -24 to 24
- head_sink_logits: float32 [32], P('tp'), may hold values from 1 to 6
- out_weight: bfloat16 [2048, 4096], P('tp'), may hold values from -0.125 to 0.125
- expert_input: bfloat16 [8192, 4096], P('ep'), may hold values from -6 to 6
- norm_gain: float32 [4096], replicated, may hold values from 0.1 to 1.9
- routing: int32 [8192, 4], P('ep'), may hold values from 0 to 63, all different within a row; in each aligned block of 128 rows (0 to 127, 128 to 255, ...) at most 12 rows name the same one
- route_weight: float32 [8192, 4], P('ep'), may hold values from 0.1 to 1
- gate_weight: bfloat16 [64, 4096, 1024], P('ep', None, 'tp'), may hold values from -0.27929688 to 0.27929688
- up_weight: bfloat16 [64, 4096, 1024], P('ep', None, 'tp'), may hold values from -0.27929688 to 0.27929688
- down_weight: bfloat16 [64, 1024, 4096], P('ep', 'tp'), may hold values from -0.046875 to 0.046875
Outputs:
- mixer_output: bfloat16 [16384, 4096], P(('ep', 'tp'))
- expert_output: bfloat16 [8192, 4096], P('ep', 'tp')
The draws below stay inside these ranges and needn't reach their ends.
Inputs may be any that keep to these rules, and one draw needn't show every extreme that they name: `projected_queries`: in the hidden draw some queries nearly equal a large multiple of a nearby key. `routing`: each row names 4 different experts; among the rows of one device (aligned blocks of 128 rows) no expert is named more than 12 times, a bound that some block reaches.
All inputs are finite; a program needn't handle non-finite values.
Results may differ from the reference program's by a relative error of at most 0.014.
Values may be sent and summed in bfloat16 or wider, within the bound.
No kernel may reach another device: no remote copies, remote signals or barrier semaphores. Data moves between devices by JAX's collectives and lax.ppermute only.
A program may use at most 128 MiB of HBM per device.

```python
import math
import jax
import jax.numpy as jnp
import numpy as np
from jax import lax

D = 4096
QUERY_HEADS = 32
KEY_VALUE_HEADS = 8
HEAD_SIZE = 64
WINDOW_KEYS = 128
FF = 1024
TOPK = 4
TOK_B_DEV = 128
EXPERTS = 64
CAP = 12
ATTENTION_TOKENS = 16384
TOKENS_B = 8192
N_EP = 64
N_TP = 4


def plant_pair(key):
    base = jax.random.fold_in(key, 17)
    leading_key, following_key = jax.random.split(base, 2)
    sampled_keys = jnp.clip(jax.random.normal(following_key, (ATTENTION_TOKENS, KEY_VALUE_HEADS, HEAD_SIZE), jnp.float32), -6.0, 6.0)
    query_vectors = jnp.clip(jax.random.normal(leading_key, (ATTENTION_TOKENS, KEY_VALUE_HEADS, QUERY_HEADS // KEY_VALUE_HEADS, HEAD_SIZE), jnp.float32), -6.0, 6.0)
    return (query_vectors.reshape(ATTENTION_TOKENS, QUERY_HEADS * HEAD_SIZE), sampled_keys.reshape(ATTENTION_TOKENS, KEY_VALUE_HEADS * HEAD_SIZE))


def draw_projected_queries(key, part):
    return plant_pair(key)[0].astype(jnp.bfloat16)


def draw_key_proj(key, part):
    return plant_pair(key)[1].astype(jnp.bfloat16)


def block_scale(own_key, extent, cuts, smallest, largest):
    factor_of, own = 1.0, jax.random.fold_in(own_key, 6)
    for dim, shards_of in cuts:
        draws = jnp.exp(jax.random.uniform(jax.random.fold_in(own, dim), (shards_of,), jnp.float32, smallest / len(cuts), largest / len(cuts)))
        factor_of = factor_of * jnp.repeat(draws, extent[dim] // shards_of).reshape([-1 if axis == dim else 1 for axis in range(len(extent))])
    return factor_of


def assign_block(key, own, number, rows, number_of, top, bound, skew):
    sequence = jax.random.permutation(key, number_of)
    heavy_load, common = shares(number_of, rows * top, bound, skew, True), shares(number_of, rows * top, bound, skew, False)
    places = jnp.arange(number_of)

    def named(tallies, rotation):
        used = int((tallies > 0).sum())
        fixed = max(1, used // 4)
        moved = fixed + (places - fixed + rotation * (used - fixed)) % max(1, number_of - fixed)
        return jnp.zeros((number_of,), jnp.int32).at[sequence[jnp.where(places < fixed, places, moved)]].set(jnp.asarray(tallies, jnp.int32))

    tallies = jnp.where(number % 4 == 0, named(heavy_load, number // 4), named(common, number - number // 4 - 1))
    mixed = jax.random.permutation(jax.random.fold_in(own, 3), number_of)
    giver, taker = mixed[0:number_of // 2 * 2:2], mixed[1:number_of // 2 * 2:2]
    room = jnp.minimum(tallies[giver] - 1, bound - tallies[taker]) // 2
    room = jnp.where((giver == sequence[0]) | (taker == sequence[0]) | (tallies[taker] == 0), 0, jnp.maximum(room, 0))
    moved = jax.random.randint(jax.random.fold_in(own, 4), (number_of // 2,), 0, 1 << 20) % (room + 1)
    tallies = tallies.at[giver].add(-moved).at[taker].add(moved)
    items = jnp.searchsorted(jnp.cumsum(tallies), jnp.arange(rows * top), side="right").astype(jnp.int32)
    table = items.reshape(top, rows).T
    table = table[jax.random.permutation(jax.random.fold_in(own, 1), rows)]
    rotation = jax.random.randint(jax.random.fold_in(own, 2), (rows, 1), 0, top)
    return jnp.take_along_axis(table, (jnp.arange(top)[None, :] + rotation) % top, axis=1)


def shares(number_of, total, limit, slope, full):
    loads = [(1 << 20) // math.isqrt(rank ** slope) + 1 for rank in range(1, number_of + 1)]
    largest = limit if full else min(limit, max(-(-total // number_of), total * loads[0] // sum(loads)))
    least = 1 if total - largest >= number_of - 1 else 0
    holding, surplus = [largest] + [least] * (number_of - 1), total - largest - least * (number_of - 1)
    while surplus > 0:
        free = [i for i in range(1, number_of) if holding[i] < largest] or [i for i in range(1, number_of) if holding[i] < limit]
        pool, remaining = sum([loads[i] for i in free]), surplus
        for i in free:
            more = min(limit - holding[i], max(1, remaining * loads[i] // pool), surplus)
            holding[i] = holding[i] + more
            surplus = surplus - more
    return np.array(holding)


def scatter_about(stream_key, shape, scale, bound, cuts=(), held_as=jnp.bfloat16):
    gain = block_scale(stream_key, shape, cuts, -0.22, 0.18) if cuts else 1.0
    drawn = jax.random.normal(stream_key, shape, jnp.float32) * scale * gain
    return jnp.minimum(jnp.maximum(drawn, -bound), bound).astype(held_as)


def setup_inputs(seed: int = 0) -> dict:
    arg_keys = jax.random.split(jax.random.key(seed), 13)
    projected_queries = draw_projected_queries(jax.random.fold_in(arg_keys[12], 71), 0)
    key_proj = draw_key_proj(jax.random.fold_in(arg_keys[12], 71), 0)
    projected_values = scatter_about(arg_keys[2], (ATTENTION_TOKENS, KEY_VALUE_HEADS * HEAD_SIZE), 4.0, 24.0, ((0, 64), (1, 4)))
    head_sink_logits = jnp.clip(1.0 + 5.0 * jax.random.uniform(arg_keys[3], (QUERY_HEADS,), jnp.float32) ** block_scale(arg_keys[3], (QUERY_HEADS,), ((0, 4),), -0.2, 0.2), 1.0, 6.0)
    out_weight = scatter_about(arg_keys[4], (QUERY_HEADS * HEAD_SIZE, D), (QUERY_HEADS * HEAD_SIZE) ** -0.5, 0.125, ((0, 4),))
    expert_input = scatter_about(arg_keys[5], (TOKENS_B, D), 1.0, 6.0, ((0, 64),))
    norm_gain = jnp.clip(1.0 + 0.18 * jax.random.normal(arg_keys[6], (D,), jnp.float32), 0.1, 1.9)
    routing_keys = jax.random.split(jax.random.fold_in(arg_keys[7], 1), TOKENS_B // TOK_B_DEV)
    routing_turns = jax.random.permutation(jax.random.fold_in(arg_keys[7], 3), TOKENS_B // TOK_B_DEV)
    routing = jax.vmap(lambda own, number: assign_block(jax.random.fold_in(arg_keys[7], 2), own, number, TOK_B_DEV, N_EP, TOPK, CAP, 2))(routing_keys, routing_turns).reshape((TOKENS_B, TOPK))
    route_weight = jnp.clip(jnp.exp(math.log(1.0) - 2.3025851 * jax.random.uniform(arg_keys[8], (TOKENS_B, TOPK), jnp.float32) ** block_scale(arg_keys[8], (TOKENS_B, TOPK), ((0, 64),), -0.2, 0.2)), 0.1, 1.0)
    gate_weight = scatter_about(arg_keys[9], (EXPERTS, D, FF), 0.046875, 0.27929688, ((0, 64), (2, 4)))
    up_weight = scatter_about(arg_keys[10], (EXPERTS, D, FF), 0.046875, 0.27929688, ((0, 64), (2, 4)))
    down_weight = scatter_about(arg_keys[11], (EXPERTS, FF, D), (16 * FF) ** -0.5, 0.046875, ((0, 64), (1, 4)))
    return {"projected_queries": projected_queries, "key_proj": key_proj, "projected_values": projected_values, "head_sink_logits": head_sink_logits, "out_weight": out_weight, "expert_input": expert_input, "norm_gain": norm_gain, "routing": routing, "route_weight": route_weight, "gate_weight": gate_weight, "up_weight": up_weight, "down_weight": down_weight}


EPS = 1e-06
CLAMP = 7.0
SLOPE = 1.702

def attend_single_head(kernel_inputs, permitted_mask):
    query_head, key_head, value_head, sink_head = kernel_inputs
    scores = jnp.einsum('nqgd,nsd->ngqs', query_head, key_head) * HEAD_SIZE ** (-0.5)
    scores = jnp.where(permitted_mask[:, None, :, :], scores, -jnp.inf)
    sink_col = sink_head[None, :, None, None]
    highest = jnp.maximum(lax.optimization_barrier(jnp.max(scores, axis=-1, keepdims=True)), sink_col)
    numerator = jnp.exp(scores - highest)
    denominator = lax.optimization_barrier(jnp.sum(numerator, axis=-1, keepdims=True)) + jnp.exp(sink_col - highest)
    weights = (numerator / denominator).astype(jnp.bfloat16)
    return jnp.einsum('ngqs,nsd->nqgd', weights.astype(jnp.float32), value_head.astype(jnp.float32))

def slot_targets(flat_ids, capacity):
    onehot = (flat_ids[:, None] == jnp.arange(N_EP, dtype=jnp.int32)[None, :]).astype(jnp.int32)
    rank_in = jnp.cumsum(onehot, axis=0) - 1
    slot_pos = lax.optimization_barrier(jnp.sum(rank_in * onehot, axis=1))
    return (flat_ids * capacity + slot_pos).astype(jnp.int32)

def reference(projected_queries, key_proj, projected_values, head_sink_logits, out_weight, expert_input, norm_gain, routing, route_weight, gate_weight, up_weight, down_weight):
    total = projected_queries.shape[0]
    count_of_blocks = total // WINDOW_KEYS
    heads_per_group = QUERY_HEADS // KEY_VALUE_HEADS
    query_vectors = projected_queries.astype(jnp.float32).reshape(count_of_blocks, WINDOW_KEYS, KEY_VALUE_HEADS, heads_per_group, HEAD_SIZE)
    blank_rows = jnp.zeros((WINDOW_KEYS, KEY_VALUE_HEADS * HEAD_SIZE), jnp.bfloat16)
    padded_keys = jnp.concatenate([blank_rows, key_proj], axis=0).astype(jnp.float32)
    padded_values = jnp.concatenate([blank_rows, projected_values], axis=0)
    window_keys = jnp.concatenate([padded_keys[:-WINDOW_KEYS].reshape(count_of_blocks, WINDOW_KEYS, KEY_VALUE_HEADS, HEAD_SIZE), padded_keys[WINDOW_KEYS:].reshape(count_of_blocks, WINDOW_KEYS, KEY_VALUE_HEADS, HEAD_SIZE)], axis=1)
    window_values = jnp.concatenate([padded_values[:-WINDOW_KEYS].reshape(count_of_blocks, WINDOW_KEYS, KEY_VALUE_HEADS, HEAD_SIZE), padded_values[WINDOW_KEYS:].reshape(count_of_blocks, WINDOW_KEYS, KEY_VALUE_HEADS, HEAD_SIZE)], axis=1)
    block_ids = jnp.arange(count_of_blocks)[:, None, None] * WINDOW_KEYS
    query_pos = block_ids + jnp.arange(WINDOW_KEYS)[None, :, None] + WINDOW_KEYS
    key_pos = block_ids + jnp.arange(2 * WINDOW_KEYS)[None, None, :]
    permitted_mask = (key_pos <= query_pos) & (query_pos - key_pos < WINDOW_KEYS) & (key_pos >= WINDOW_KEYS)
    head_outputs = lax.map(lambda kernel_inputs: attend_single_head(kernel_inputs, permitted_mask), (query_vectors.transpose(2, 0, 1, 3, 4), window_keys.transpose(2, 0, 1, 3), window_values.transpose(2, 0, 1, 3), head_sink_logits.reshape(KEY_VALUE_HEADS, heads_per_group)))
    attended = head_outputs.transpose(1, 2, 0, 3, 4).reshape(total, QUERY_HEADS * HEAD_SIZE).astype(jnp.bfloat16)
    head_share = QUERY_HEADS * HEAD_SIZE // N_TP
    summed = jnp.zeros((total, D), jnp.float32)
    for group in range(N_TP):
        partial_value = jnp.dot(attended[:, group * head_share:(group + 1) * head_share], out_weight[group * head_share:(group + 1) * head_share], preferred_element_type=jnp.float32).astype(jnp.bfloat16)
        summed = summed + lax.optimization_barrier(partial_value).astype(jnp.float32)
    mixer_output = summed.astype(jnp.bfloat16)
    capacity = CAP
    widened = expert_input.astype(jnp.float32)
    normed = (widened * lax.rsqrt(lax.optimization_barrier(jnp.mean(widened * widened, axis=-1, keepdims=True)) + EPS) * norm_gain[None, :]).astype(jnp.bfloat16)
    per_source = TOK_B_DEV * TOPK
    flat_ids = routing.reshape(N_EP, per_source).astype(jnp.int32)
    target = jax.vmap(lambda id_row: slot_targets(id_row, capacity))(flat_ids)
    tok_ids = (jnp.arange(per_source) // TOPK).astype(jnp.int32)
    slot_tok = jax.vmap(lambda tgt_row: jnp.full((N_EP * capacity,), TOK_B_DEV, jnp.int32).at[tgt_row].set(tok_ids))(target)
    extended = jnp.concatenate([normed.reshape(N_EP, TOK_B_DEV, D), jnp.zeros((N_EP, 1, D), jnp.bfloat16)], axis=1)

    def run_expert(expert_id):
        picks = lax.dynamic_slice_in_dim(slot_tok, expert_id * capacity, capacity, 1)
        expert_rows = jax.vmap(lambda block_rows, pick_row: jnp.take(block_rows, pick_row, axis=0))(extended, picks)
        expert_rows = expert_rows.reshape(N_EP * capacity, D)
        gate_pre = jnp.dot(expert_rows, gate_weight[expert_id], preferred_element_type=jnp.float32)
        up_pre = jnp.dot(expert_rows, up_weight[expert_id], preferred_element_type=jnp.float32)
        gate_cut = jnp.minimum(gate_pre, CLAMP)
        activated = ((jnp.clip(up_pre, -CLAMP, CLAMP) + 1.0) * gate_cut * jax.nn.sigmoid(SLOPE * gate_cut)).astype(jnp.bfloat16)
        return jnp.dot(activated, down_weight[expert_id], preferred_element_type=jnp.float32).astype(jnp.bfloat16)
    results = lax.map(run_expert, jnp.arange(N_EP, dtype=jnp.int32))
    source = jnp.arange(N_EP, dtype=jnp.int32)[:, None]
    slot_of = target - flat_ids * capacity
    gather_at = ((flat_ids * N_EP + source) * capacity + slot_of).astype(jnp.int32)
    picked = jnp.take(results.reshape(-1, D), gather_at.reshape(-1), axis=0).astype(jnp.float32)
    picked = picked.reshape(N_EP * TOK_B_DEV, TOPK, D)
    expert_output = lax.optimization_barrier(jnp.sum(picked * route_weight[:, :, None], axis=1)).astype(jnp.bfloat16)
    return (mixer_output, expert_output)
```

```python
import jax
import jax.numpy as jnp
from jax import lax
from jax.sharding import PartitionSpec as P

D = 4096
HEAD_SIZE = 64
WINDOW_KEYS = 128
TOPK = 4
EPS = 1e-06
CLAMP = 7.0
SLOPE = 1.702
N_TP = 4


def passed_along(block, axis, distance):
    devices = range(lax.axis_size(axis))
    route = [(i - distance, i) for i in devices if i - distance in devices]
    return lax.ppermute(block, axis, route)


def shifted(block, distance):
    return lax.ppermute(block, "tp", [((i + distance) % N_TP, i) for i in range(N_TP)])


def gathered(block):
    half = block.shape[0] // 2
    nxt = shifted(block, 1)
    prv = shifted(block, -1)
    far_a = shifted(nxt[:half], 1)
    far_b = shifted(prv[half:], -1)
    return block, nxt, jnp.concatenate([far_a, far_b], axis=0), prv


def dot(a, b):
    return jnp.dot(a, b, preferred_element_type=jnp.float32)


def attention(projected_queries, key_proj, projected_values, head_sink_logits):
    query_rows = projected_queries.shape[0]
    kv_heads = key_proj.shape[1] // HEAD_SIZE
    heads_per_group = projected_queries.shape[1] // HEAD_SIZE // kv_heads
    count_of_blocks = query_rows // WINDOW_KEYS
    prior_key, prior_value = passed_along(
        (key_proj[query_rows - WINDOW_KEYS :], projected_values[query_rows - WINDOW_KEYS :]),
        "ep",
        1,
    )
    key_all = jnp.concatenate([prior_key, key_proj], axis=0)
    value_all = jnp.concatenate([prior_value, projected_values], axis=0)
    window_keys = jnp.concatenate(
        [
            key_all[:-WINDOW_KEYS].reshape(count_of_blocks, WINDOW_KEYS, kv_heads, HEAD_SIZE),
            key_all[WINDOW_KEYS:].reshape(count_of_blocks, WINDOW_KEYS, kv_heads, HEAD_SIZE),
        ],
        axis=1,
    )
    window_values = jnp.concatenate(
        [
            value_all[:-WINDOW_KEYS].reshape(count_of_blocks, WINDOW_KEYS, kv_heads, HEAD_SIZE),
            value_all[WINDOW_KEYS:].reshape(count_of_blocks, WINDOW_KEYS, kv_heads, HEAD_SIZE),
        ],
        axis=1,
    )
    query_blocks = projected_queries.reshape(
        count_of_blocks, WINDOW_KEYS, kv_heads, heads_per_group, HEAD_SIZE
    )
    scores = jnp.einsum(
        "nqhgd,nshd->nhgqs", query_blocks, window_keys, preferred_element_type=jnp.float32
    ) * HEAD_SIZE ** (-0.5)
    offset = lax.axis_index("ep") * query_rows
    block_ids = jnp.arange(count_of_blocks)[:, None, None] * WINDOW_KEYS + offset
    query_pos = block_ids + jnp.arange(WINDOW_KEYS)[None, :, None]
    key_pos = block_ids - WINDOW_KEYS + jnp.arange(2 * WINDOW_KEYS)[None, None, :]
    permitted_mask = (key_pos <= query_pos) & (query_pos - key_pos < WINDOW_KEYS) & (key_pos >= 0)
    scores = jnp.where(permitted_mask[:, None, None, :, :], scores, -jnp.inf)
    sink_col = head_sink_logits.reshape(kv_heads, heads_per_group)[None, :, :, None, None]
    highest = jnp.maximum(jnp.max(scores, axis=-1, keepdims=True), sink_col)
    numerator = jnp.exp(scores - highest)
    denominator = jnp.sum(numerator, axis=-1, keepdims=True) + jnp.exp(sink_col - highest)
    weights = (numerator / denominator).astype(jnp.bfloat16)
    attended = jnp.einsum(
        "nhgqs,nshd->nqhgd", weights, window_values, preferred_element_type=jnp.float32
    )
    return attended.astype(jnp.bfloat16).reshape(
        query_rows, kv_heads * heads_per_group * HEAD_SIZE
    )


def shards(
    projected_queries,
    key_proj,
    projected_values,
    head_sink_logits,
    out_weight,
    expert_input,
    norm_gain,
    routing,
    route_weight,
    gate_weight,
    up_weight,
    down_weight,
):
    bf = jnp.bfloat16
    tp = lax.axis_index("tp")
    token_rows = expert_input.shape[0]
    experts = lax.axis_size("ep")
    capacity = 3 * token_rows * TOPK // (2 * experts)
    share = D // N_TP
    half = share // 2

    down_own = down_weight[0]
    down_parts = [None] * N_TP
    for k in range(N_TP):
        block = lax.dynamic_slice_in_dim(down_own, ((tp + N_TP - k) % N_TP) * share, share, 1)
        down_parts[k] = shifted(block, k) if k else block

    ids = routing.T.reshape(-1)
    same = (ids[:, None] == ids[None, :]) & (
        jnp.arange(ids.shape[0])[:, None] < jnp.arange(ids.shape[0])[None, :]
    )
    rank = jnp.sum(same.astype(jnp.int32), axis=0)
    target = (ids * 16 + rank).reshape(TOPK, token_rows)
    row8 = jnp.arange(experts * 8)
    slot_low = (row8 // 8) * 16 + row8 % 8
    slot_high = (row8 // 8) * 16 + 8 + row8 % 4
    upper = (row8 % 8) >= 4

    def named(slot):
        hit = slot[:, None] == target[0][None, :]
        for k in range(1, TOPK):
            hit = hit | (slot[:, None] == target[k][None, :])
        return hit

    pick_low = named(slot_low).astype(bf)
    pick_high = named(slot_high)
    pick_high = jnp.concatenate(
        [(pick_high & ~upper[:, None]).astype(bf), (pick_high & upper[:, None]).astype(bf)], axis=1
    )

    widened = expert_input.astype(jnp.float32)
    scale = lax.rsqrt(jnp.mean(widened * widened, axis=-1, keepdims=True) + EPS)
    own = lax.dynamic_slice_in_dim(expert_input, tp * share, share, 1).astype(jnp.float32)
    gain = lax.dynamic_slice_in_dim(norm_gain, tp * share, share, 0)
    normed = (own * scale * gain[None, :]).astype(bf)
    left, right = normed[:, :half], normed[:, half:]

    def exchanged(block):
        return lax.all_to_all(block, "ep", split_axis=0, concat_axis=0, tiled=True)

    sent_a = dot(pick_low, left).astype(bf)
    sent_b = dot(pick_low, right).astype(bf)
    sent_c = dot(pick_high, jnp.concatenate([left, right], axis=0)).astype(bf)
    got_a = exchanged(sent_a)
    got_b = exchanged(sent_b)
    got_c = exchanged(sent_c)

    gate_one, up_one = gate_weight[0], up_weight[0]

    def rows_of(weight, k, first, count):
        return lax.dynamic_slice_in_dim(weight, ((tp + k) % N_TP) * share + first, count, 0)

    def activate(gate_pre, up_pre):
        gate_cut = jnp.minimum(gate_pre, CLAMP)
        return (
            (jnp.clip(up_pre, -CLAMP, CLAMP) + 1.0) * gate_cut * jax.nn.sigmoid(SLOPE * gate_cut)
        ).astype(bf)

    parts_a = gathered(got_a)
    parts_b = gathered(got_b)
    parts_c = gathered(got_c)

    def total(terms):
        out = terms[0]
        for term in terms[1:]:
            out = out + term
        return out

    order = (0, 1, 3, 2)
    gate_low = total(
        [dot(parts_a[k], rows_of(gate_one, k, 0, half)) for k in order]
        + [dot(parts_b[k], rows_of(gate_one, k, half, half)) for k in order]
    )
    up_low = total(
        [dot(parts_a[k], rows_of(up_one, k, 0, half)) for k in order]
        + [dot(parts_b[k], rows_of(up_one, k, half, half)) for k in order]
    )
    act_low = gathered(activate(gate_low, up_low))

    def joined(block):
        return block.reshape(experts, 2, 4, half).transpose(0, 2, 1, 3).reshape(experts * 4, share)

    joined_c = [joined(p) for p in parts_c]
    gate_high = total([dot(joined_c[k], rows_of(gate_one, k, 0, share)) for k in order])
    up_high = total([dot(joined_c[k], rows_of(up_one, k, 0, share)) for k in order])
    act_high = gathered(activate(gate_high, up_high))

    result_low = total([dot(act_low[k], down_parts[k]) for k in order]).astype(bf)
    back_low = exchanged(result_low)
    result_high = total([dot(act_high[k], down_parts[k]) for k in order]).astype(bf)
    result_high = (
        result_high.reshape(experts, 4, 2, half).transpose(0, 2, 1, 3).reshape(experts * 8, half)
    )
    back_high = exchanged(result_high)

    attended = attention(projected_queries, key_proj, projected_values, head_sink_logits)
    partial = dot(attended, out_weight).astype(bf)
    owned = partial.shape[0] // N_TP
    mixed = None
    for k in range(N_TP):
        block = lax.dynamic_slice_in_dim(partial, ((tp + N_TP - k) % N_TP) * owned, owned, 0)
        block = (shifted(block, k) if k else block).astype(jnp.float32)
        mixed = block if mixed is None else mixed + block
    mixer_output = mixed.astype(bf)

    def combining(slot):
        out = None
        for k in range(TOPK):
            term = jnp.where(target[k][:, None] == slot[None, :], route_weight[:, k][:, None], 0.0)
            out = term if out is None else out + term
        rounded = lax.reduce_precision(out, 8, 7)
        return rounded.astype(bf), (out - rounded).astype(bf)

    low_main, low_rest = combining(slot_low)
    high_main, high_rest = combining(slot_high)
    zero = jnp.zeros((), bf)
    out_low = dot(low_main, back_low) + dot(low_rest, back_low)
    lower_main = jnp.where(upper[None, :], zero, high_main)
    lower_rest = jnp.where(upper[None, :], zero, high_rest)
    upper_main = jnp.where(upper[None, :], high_main, zero)
    upper_rest = jnp.where(upper[None, :], high_rest, zero)
    out_left = dot(lower_main, back_high) + dot(lower_rest, back_high)
    out_right = dot(upper_main, back_high) + dot(upper_rest, back_high)
    expert_output = (out_low + jnp.concatenate([out_left, out_right], axis=1)).astype(bf)
    return (mixer_output, expert_output)


def solution(mesh):
    placed = (
        P("ep", "tp"),
        P("ep", "tp"),
        P("ep", "tp"),
        P("tp"),
        P("tp", None),
        P("ep", None),
        P(),
        P("ep", None),
        P("ep", None),
        P("ep", None, "tp"),
        P("ep", None, "tp"),
        P("ep", "tp", None),
    )
    return jax.shard_map(
        shards,
        mesh=mesh,
        in_specs=placed,
        out_specs=(P(("ep", "tp"), None), P("ep", "tp")),
        check_vma=False,
    )
```

```python
import functools

import jax
import jax.numpy as jnp
from jax import lax
from jax.experimental import pallas as pl
from jax.experimental.pallas import tpu as pltpu
from jax.sharding import PartitionSpec as P

D = 4096
HEAD_SIZE = 64
WINDOW_KEYS = 128
TOPK = 4
EPS = 1e-06
CLAMP = 7.0
SLOPE = 1.702
N_TP = 4
SLOTS = 4


def shifted(block, distance):
    return lax.ppermute(block, "tp", [((i + distance) % N_TP, i) for i in range(N_TP)])


def passed_along(block):
    devices = lax.axis_size("ep")
    return lax.ppermute(block, "ep", [(i, i + 1) for i in range(devices - 1)])


def exchanged(block):
    return lax.all_to_all(block, "ep", split_axis=0, concat_axis=0, tiled=True)


def dot(a, b):
    return jnp.dot(a, b, preferred_element_type=jnp.float32)


def attention(projected_queries, key_proj, projected_values, head_sink_logits):
    query_rows = projected_queries.shape[0]
    kv_heads = key_proj.shape[1] // HEAD_SIZE
    heads_per_group = projected_queries.shape[1] // HEAD_SIZE // kv_heads
    count_of_blocks = query_rows // WINDOW_KEYS
    prior_key = passed_along(key_proj[query_rows - WINDOW_KEYS :])
    prior_value = passed_along(projected_values[query_rows - WINDOW_KEYS :])
    key_all = jnp.concatenate([prior_key, key_proj], axis=0)
    value_all = jnp.concatenate([prior_value, projected_values], axis=0)
    window_keys = jnp.concatenate(
        [
            key_all[:-WINDOW_KEYS].reshape(count_of_blocks, WINDOW_KEYS, kv_heads, HEAD_SIZE),
            key_all[WINDOW_KEYS:].reshape(count_of_blocks, WINDOW_KEYS, kv_heads, HEAD_SIZE),
        ],
        axis=1,
    )
    window_values = jnp.concatenate(
        [
            value_all[:-WINDOW_KEYS].reshape(count_of_blocks, WINDOW_KEYS, kv_heads, HEAD_SIZE),
            value_all[WINDOW_KEYS:].reshape(count_of_blocks, WINDOW_KEYS, kv_heads, HEAD_SIZE),
        ],
        axis=1,
    )
    query_blocks = projected_queries.reshape(
        count_of_blocks, WINDOW_KEYS, kv_heads, heads_per_group, HEAD_SIZE
    )
    scores = jnp.einsum(
        "nqhgd,nshd->nhgqs", query_blocks, window_keys, preferred_element_type=jnp.float32
    ) * HEAD_SIZE ** (-0.5)
    offset = lax.axis_index("ep") * query_rows
    block_ids = jnp.arange(count_of_blocks)[:, None, None] * WINDOW_KEYS + offset
    query_pos = block_ids + jnp.arange(WINDOW_KEYS)[None, :, None]
    key_pos = block_ids - WINDOW_KEYS + jnp.arange(2 * WINDOW_KEYS)[None, None, :]
    permitted_mask = (key_pos <= query_pos) & (query_pos - key_pos < WINDOW_KEYS) & (key_pos >= 0)
    scores = jnp.where(permitted_mask[:, None, None, :, :], scores, -jnp.inf)
    sink_col = head_sink_logits.reshape(kv_heads, heads_per_group)[None, :, :, None, None]
    highest = jnp.maximum(jnp.max(scores, axis=-1, keepdims=True), sink_col)
    numerator = jnp.exp(scores - highest)
    denominator = jnp.sum(numerator, axis=-1, keepdims=True) + jnp.exp(sink_col - highest)
    weights = (numerator / denominator).astype(jnp.bfloat16)
    attended = jnp.einsum(
        "nhgqs,nshd->nqhgd", weights, window_values, preferred_element_type=jnp.float32
    )
    return attended.astype(jnp.bfloat16).reshape(
        query_rows, kv_heads * heads_per_group * HEAD_SIZE
    )


def _lower_rows(shape):
    return lax.broadcasted_iota(jnp.int32, shape, 1) < SLOTS


def hidden_kernel(far_count, tp_ref, own, nxt, *refs):
    far = refs[:far_count]
    prv, gate_ref, up_ref, out_ref, zg0, zg1, zu0, zu1 = refs[far_count:]
    step = pl.program_id(0)
    rows, width = own.shape

    def add(first, block):
        count = block.shape[0]
        at = pl.ds(first, count)
        for acc, w_ref, low in ((zg0, gate_ref, 0), (zg1, gate_ref, 1), (zu0, up_ref, 0), (zu1, up_ref, 1)):
            acc[at, :] += dot(block, w_ref[low * width : (low + 1) * width, :])

    @pl.when(step == 0)
    def _():
        for acc, w_ref, low in ((zg0, gate_ref, 0), (zg1, gate_ref, 1), (zu0, up_ref, 0), (zu1, up_ref, 1)):
            acc[...] = dot(own[...], w_ref[low * width : (low + 1) * width, :])

    @pl.when(step == 1)
    def _():
        add(0, nxt[...])

    @pl.when(step == 2)
    def _():
        for k in range(far_count):
            add(k * (rows // far_count), far[k][...])

    @pl.when(step == 3)
    def _():
        add(0, prv[...])
        cols = zg0.shape[1]
        groups = rows // 8

        def paired(z0, z1):
            left = z0[...].reshape(groups, 8, cols)
            right = z1[...].reshape(groups, 8, cols)
            h = groups // 2
            first = left[:h] + pltpu.roll(right[:h], SLOTS, 1)
            second = pltpu.roll(left[h:], SLOTS, 1) + right[h:]
            return jnp.where(_lower_rows(first.shape), first, second).reshape(h * 8, cols)

        gate_cut = jnp.minimum(paired(zg0, zg1), CLAMP)
        up_cut = jnp.clip(paired(zu0, zu1), -CLAMP, CLAMP)
        out_ref[...] = ((up_cut + 1.0) * gate_cut * jax.nn.sigmoid(SLOPE * gate_cut)).astype(out_ref.dtype)


def hidden(tp, own, nxt, far, prv, gate, up):
    rows, width = own.shape
    cols = gate.shape[1]
    whole = pl.BlockSpec((rows, width), lambda j, t: (0, 0))
    part = pl.BlockSpec((rows // len(far), width), lambda j, t: (0, 0))
    weight = pl.BlockSpec((2 * width, cols), lambda j, t: ((t[0] + j) % N_TP, 0))
    return pl.pallas_call(
        functools.partial(hidden_kernel, len(far)),
        grid_spec=pltpu.PrefetchScalarGridSpec(
            num_scalar_prefetch=1,
            grid=(N_TP,),
            in_specs=[whole, whole] + [part] * len(far) + [whole, weight, weight],
            out_specs=pl.BlockSpec((rows // 2, cols), lambda j, t: (0, 0)),
            scratch_shapes=[pltpu.VMEM((rows, cols), jnp.float32)] * 4,
        ),
        out_shape=jax.ShapeDtypeStruct((rows // 2, cols), jnp.bfloat16),
        cost_estimate=pl.CostEstimate(flops=2 * rows * 4096 * 512, bytes_accessed=6 << 20, transcendentals=0),
        name="hidden",
    )(tp, own, nxt, *far, prv, gate, up)


def result_kernel(chunks, *refs):
    acts = refs[: 4 * chunks]
    downs = refs[4 * chunks : 4 * chunks + 4]
    out_ref = refs[4 * chunks + 4]
    rows = acts[0].shape[0]
    half = downs[0].shape[1] // 2
    for c in range(chunks):
        res = dot(acts[4 * c][...], downs[0][...])
        for k in range(1, 4):
            res = res + dot(acts[4 * c + k][...], downs[k][...])
        left = res[:, :half].reshape(rows // 8, 8, half)
        right = res[:, half:].reshape(rows // 8, 8, half)
        low = _lower_rows(left.shape)
        first = jnp.where(low, left, pltpu.roll(right, SLOTS, 1)).reshape(rows, half)
        second = jnp.where(low, pltpu.roll(left, SLOTS, 1), right).reshape(rows, half)
        out_ref[:rows, c * half : (c + 1) * half] = first.astype(out_ref.dtype)
        out_ref[rows:, c * half : (c + 1) * half] = second.astype(out_ref.dtype)


def results(acts, downs):
    chunks = len(acts)
    rows = acts[0][0].shape[0]
    cols = downs[0].shape[1]
    flat = [a for chunk in acts for a in chunk]
    return pl.pallas_call(
        functools.partial(result_kernel, chunks),
        out_shape=jax.ShapeDtypeStruct((2 * rows, chunks * cols // 2), jnp.bfloat16),
        cost_estimate=pl.CostEstimate(
            flops=chunks * 2 * rows * 1024 * cols, bytes_accessed=3 << 20, transcendentals=0
        ),
        name="results",
    )(*flat, *downs)


def combine_kernel(target_ref, weight_ref, first_ref, rest_ref, out_ref):
    tokens = target_ref.shape[0]
    rows, half = first_ref.shape
    left = jnp.zeros((tokens, half), jnp.float32)
    right = jnp.zeros((tokens, half), jnp.float32)
    lane = lax.broadcasted_iota(jnp.int32, (tokens, rows), 1)
    for c in range(3):
        slot = (lane // 8) * 16 + SLOTS * c + lane % SLOTS
        mix = jnp.zeros((tokens, rows), jnp.float32)
        for k in range(TOPK):
            mix = jnp.where(target_ref[:, k : k + 1] == slot, weight_ref[:, k : k + 1], mix)
        main = mix.astype(jnp.bfloat16).astype(jnp.float32)
        rest = mix - main
        block = first_ref[...] if c == 0 else rest_ref[:, (c - 1) * half : c * half]
        low = lane % 8 < SLOTS
        for term in (main, rest):
            left += dot(jnp.where(low, term, 0.0).astype(jnp.bfloat16), block)
            right += dot(jnp.where(low, 0.0, term).astype(jnp.bfloat16), block)
    out_ref[:, :half] = left.astype(out_ref.dtype)
    out_ref[:, half:] = right.astype(out_ref.dtype)


def combined(target, weight, first, rest):
    tokens = target.shape[0]
    return pl.pallas_call(
        combine_kernel,
        out_shape=jax.ShapeDtypeStruct((tokens, 2 * first.shape[1]), jnp.bfloat16),
        cost_estimate=pl.CostEstimate(flops=10**9, bytes_accessed=3 << 20, transcendentals=0),
        name="combine",
    )(target, weight, first, rest)


def program(
    projected_queries,
    key_proj,
    projected_values,
    head_sink_logits,
    out_weight,
    expert_input,
    norm_gain,
    routing,
    route_weight,
    gate_weight,
    up_weight,
    down_weight,
):
    bf = jnp.bfloat16
    tp = lax.axis_index("tp")
    at = tp.astype(jnp.int32).reshape(1)
    token_rows = expert_input.shape[0]
    experts = lax.axis_size("ep")
    share = D // N_TP
    half = share // 2

    ids = routing.T.reshape(-1)
    place = jnp.arange(ids.shape[0])
    same = (ids[:, None] == ids[None, :]) & (place[:, None] < place[None, :])
    rank = jnp.sum(same.astype(jnp.int32), axis=0)
    target = (ids * 16 + rank).reshape(TOPK, token_rows)

    widened = expert_input.astype(jnp.float32)
    scale = lax.rsqrt(jnp.mean(widened * widened, axis=-1, keepdims=True) + EPS)
    own = lax.dynamic_slice_in_dim(expert_input, tp * share, share, 1).astype(jnp.float32)
    gain = lax.dynamic_slice_in_dim(norm_gain, tp * share, share, 0)
    normed = (own * scale * gain[None, :]).astype(bf)
    stacked = jnp.concatenate([normed[:, :half], normed[:, half:]], axis=0)

    row8 = jnp.arange(experts * 8)
    upper = (row8 % 8) >= SLOTS

    def sent(c):
        slot = (row8 // 8) * 16 + SLOTS * c + row8 % SLOTS
        hit = slot[:, None] == target[0][None, :]
        for k in range(1, TOPK):
            hit = hit | (slot[:, None] == target[k][None, :])
        pick = jnp.concatenate([hit & ~upper[:, None], hit & upper[:, None]], axis=1).astype(bf)
        return dot(pick, stacked).astype(bf)

    got1 = exchanged(sent(0))
    got2 = exchanged(sent(1))
    got3 = exchanged(sent(2))

    down_parts = []
    for k in range(N_TP):
        block = lax.dynamic_slice_in_dim(down_weight[0], ((tp + N_TP - k) % N_TP) * share, share, 1)
        down_parts.append(shifted(block, k) if k else block)

    gate_one, up_one = gate_weight[0], up_weight[0]

    nxt1, prv1 = shifted(got1, 1), shifted(got1, -1)
    far1 = shifted(nxt1, 1)
    nxt2, prv2 = shifted(got2, 1), shifted(got2, -1)
    far2 = shifted(prv2, -1)
    nxt3, prv3 = shifted(got3, 1), shifted(got3, -1)
    mid = got3.shape[0] // 2
    far3 = (shifted(nxt3[:mid], 1), shifted(prv3[mid:], -1))

    act1 = hidden(at, got1, nxt1, (far1,), prv1, gate_one, up_one)
    act2 = hidden(at, got2, nxt2, (far2,), prv2, gate_one, up_one)
    act3 = hidden(at, got3, nxt3, far3, prv3, gate_one, up_one)

    def spread(act):
        return (act, shifted(act, 1), shifted(act, 2), shifted(act, -1))

    back1 = exchanged(results((spread(act1),), down_parts))
    back2 = exchanged(results((spread(act2), spread(act3)), down_parts))

    attended = attention(projected_queries, key_proj, projected_values, head_sink_logits)
    partial = dot(attended, out_weight).astype(bf)
    owned = partial.shape[0] // N_TP
    mixed = None
    for k in range(N_TP):
        block = lax.dynamic_slice_in_dim(partial, ((tp + N_TP - k) % N_TP) * owned, owned, 0)
        block = (shifted(block, k) if k else block).astype(jnp.float32)
        mixed = block if mixed is None else mixed + block
    mixer_output = mixed.astype(bf)

    expert_output = combined(target.T, route_weight, back1, back2)
    return (mixer_output, expert_output)


def solution(mesh):
    placed = (
        P("ep", "tp"),
        P("ep", "tp"),
        P("ep", "tp"),
        P("tp"),
        P("tp", None),
        P("ep", None),
        P(),
        P("ep", None),
        P("ep", None),
        P("ep", None, "tp"),
        P("ep", None, "tp"),
        P("ep", "tp", None),
    )
    return jax.shard_map(
        program,
        mesh=mesh,
        in_specs=placed,
        out_specs=(P(("ep", "tp"), None), P("ep", "tp")),
        check_vma=False,
    )
```

```python
import functools

import jax
import jax.numpy as jnp
from jax import lax
from jax.experimental import pallas as pl
from jax.experimental.pallas import tpu as pltpu
from jax.sharding import PartitionSpec as P

D = 4096
HEAD_SIZE = 64
WINDOW_KEYS = 128
TOPK = 4
EPS = 1e-06
CLAMP = 7.0
SLOPE = 1.702
N_TP = 4
SLOTS = 6
LANES = 256
BLOCKS = 3


def shifted(block, distance):
    return lax.ppermute(block, "tp", [((i + distance) % N_TP, i) for i in range(N_TP)])


def exchanged(block):
    return lax.all_to_all(block, "ep", split_axis=0, concat_axis=0, tiled=True)


def dot(a, b):
    return jnp.dot(a, b, preferred_element_type=jnp.float32)


def attention(projected_queries, key_proj, projected_values, head_sink_logits):
    query_rows = projected_queries.shape[0]
    kv_heads = key_proj.shape[1] // HEAD_SIZE
    heads_per_group = projected_queries.shape[1] // HEAD_SIZE // kv_heads
    count_of_blocks = query_rows // WINDOW_KEYS
    kept = key_proj.shape[1]
    prior = lax.ppermute(
        jnp.concatenate(
            [key_proj[query_rows - WINDOW_KEYS :], projected_values[query_rows - WINDOW_KEYS :]],
            axis=1,
        ),
        "ep",
        [(i, i + 1) for i in range(lax.axis_size("ep") - 1)],
    )
    prior_key, prior_value = prior[:, :kept], prior[:, kept:]
    key_all = jnp.concatenate([prior_key, key_proj], axis=0)
    value_all = jnp.concatenate([prior_value, projected_values], axis=0)
    window_keys = jnp.concatenate(
        [
            key_all[:-WINDOW_KEYS].reshape(count_of_blocks, WINDOW_KEYS, kv_heads, HEAD_SIZE),
            key_all[WINDOW_KEYS:].reshape(count_of_blocks, WINDOW_KEYS, kv_heads, HEAD_SIZE),
        ],
        axis=1,
    )
    window_values = jnp.concatenate(
        [
            value_all[:-WINDOW_KEYS].reshape(count_of_blocks, WINDOW_KEYS, kv_heads, HEAD_SIZE),
            value_all[WINDOW_KEYS:].reshape(count_of_blocks, WINDOW_KEYS, kv_heads, HEAD_SIZE),
        ],
        axis=1,
    )
    query_blocks = projected_queries.reshape(
        count_of_blocks, WINDOW_KEYS, kv_heads, heads_per_group, HEAD_SIZE
    )
    scores = jnp.einsum(
        "nqhgd,nshd->nhgqs", query_blocks, window_keys, preferred_element_type=jnp.float32
    ) * HEAD_SIZE ** (-0.5)
    offset = lax.axis_index("ep") * query_rows
    block_ids = jnp.arange(count_of_blocks)[:, None, None] * WINDOW_KEYS + offset
    query_pos = block_ids + jnp.arange(WINDOW_KEYS)[None, :, None]
    key_pos = block_ids - WINDOW_KEYS + jnp.arange(2 * WINDOW_KEYS)[None, None, :]
    permitted_mask = (key_pos <= query_pos) & (query_pos - key_pos < WINDOW_KEYS) & (key_pos >= 0)
    scores = jnp.where(permitted_mask[:, None, None, :, :], scores, -jnp.inf)
    sink_col = head_sink_logits.reshape(kv_heads, heads_per_group)[None, :, :, None, None]
    highest = jnp.maximum(jnp.max(scores, axis=-1, keepdims=True), sink_col)
    numerator = jnp.exp(scores - highest)
    denominator = jnp.sum(numerator, axis=-1, keepdims=True) + jnp.exp(sink_col - highest)
    weights = (numerator / denominator).astype(jnp.bfloat16)
    attended = jnp.einsum(
        "nhgqs,nshd->nqhgd", weights, window_values, preferred_element_type=jnp.float32
    )
    return attended.astype(jnp.bfloat16).reshape(
        query_rows, kv_heads * heads_per_group * HEAD_SIZE
    )


def params(mib):
    return pltpu.CompilerParams(vmem_limit_bytes=mib << 20)


def cost(flops, size):
    return pl.CostEstimate(flops=flops, bytes_accessed=size, transcendentals=0)


def dispatch_kernel(chunk_ref, target_ref, normed_ref, out_ref):
    rows = out_ref.shape[0]
    tokens = normed_ref.shape[0]
    row = lax.broadcasted_iota(jnp.int32, (rows, tokens), 0)
    place = row % 8
    first = (row // 8) * 16 + chunk_ref[0] * SLOTS

    def picks(slot):
        hit = target_ref[0:1, :] == slot
        for k in range(1, TOPK):
            hit = hit | (target_ref[k : k + 1, :] == slot)
        return jnp.where(hit, 1.0, 0.0).astype(jnp.bfloat16)

    main = picks(jnp.where(place < SLOTS, first + place, -1))
    last = normed_ref[:, BLOCKS * LANES :]
    for b in range(BLOCKS):
        extra = picks(jnp.where(place < SLOTS, -1, first + 2 * b + place - SLOTS))
        cols = slice(b * LANES, (b + 1) * LANES)
        out_ref[:, cols] = (dot(main, normed_ref[:, cols]) + dot(extra, last)).astype(out_ref.dtype)


def dispatched(chunk, target, normed, rows):
    vmem = pl.BlockSpec(memory_space=pltpu.VMEM)
    return pl.pallas_call(
        dispatch_kernel,
        in_specs=[pl.BlockSpec(memory_space=pltpu.SMEM), vmem, vmem],
        out_specs=vmem,
        out_shape=jax.ShapeDtypeStruct((rows, BLOCKS * LANES), jnp.bfloat16),
        compiler_params=params(12),
        cost_estimate=cost(4 * rows * 128 * 768, 1 << 20),
        name="dispatch",
    )(jnp.full((1,), chunk, jnp.int32), target, normed)


def hidden_kernel(tp_ref, own, nt, nb, ft, fb, pt, pb, gate_ref, up_ref, out_ref, acc):
    step = pl.program_id(0)
    rows = own.shape[0]
    width = BLOCKS * LANES

    def put(at, block, fresh):
        for side, w_ref in enumerate((gate_ref, up_ref)):
            terms = [dot(block, w_ref[:width, :])]
            for b in range(BLOCKS):
                terms.append(dot(block[:, b * LANES : (b + 1) * LANES], w_ref[width:, :]))
            for k, term in enumerate(terms):
                if fresh:
                    acc[4 * side + k, at, :] = term
                else:
                    acc[4 * side + k, at, :] += term

    @pl.when(step == 0)
    def _():
        put(pl.ds(0, rows), own[...], True)

    for j, (top, bottom) in enumerate(((nt, nb), (ft, fb), (pt, pb))):

        @pl.when(step == j + 1)
        def _():
            put(pl.ds(0, rows // 2), top[...], False)
            put(pl.ds(rows // 2, rows // 2), bottom[...], False)

    @pl.when(step == N_TP - 1)
    def _():
        shape = (rows // 8, 8, LANES)
        place = lax.broadcasted_iota(jnp.int32, shape, 1)

        def whole(side):
            moved = [
                pltpu.roll(acc[4 * side + 1 + b].reshape(shape), 2 * b + 2, 1) for b in range(BLOCKS)
            ]
            extra = jnp.where(place < 2, moved[0], jnp.where(place < 4, moved[1], moved[2]))
            return (acc[4 * side].reshape(shape) + extra).reshape(rows, LANES)

        gate_cut = jnp.minimum(whole(0), CLAMP)
        up_cut = jnp.clip(whole(1), -CLAMP, CLAMP)
        out_ref[...] = ((up_cut + 1.0) * gate_cut * jax.nn.sigmoid(SLOPE * gate_cut)).astype(
            out_ref.dtype
        )


def hidden(tp, own, pieces, gate, up):
    rows, width = own.shape
    cols = gate.shape[1]
    half = pl.BlockSpec((rows // 2, width), lambda j, t: (0, 0))
    weight = pl.BlockSpec((width + LANES, cols), lambda j, t: ((t[0] + j) % N_TP, 0))
    return pl.pallas_call(
        hidden_kernel,
        grid_spec=pltpu.PrefetchScalarGridSpec(
            num_scalar_prefetch=1,
            grid=(N_TP,),
            in_specs=[pl.BlockSpec((rows, width), lambda j, t: (0, 0))] + [half] * 6 + [weight] * 2,
            out_specs=pl.BlockSpec((rows, cols), lambda j, t: (0, 0)),
            scratch_shapes=[pltpu.VMEM((8, rows, cols), jnp.float32)],
        ),
        out_shape=jax.ShapeDtypeStruct((rows, cols), jnp.bfloat16),
        compiler_params=params(24),
        cost_estimate=cost(16 * rows * width * cols, 8 << 20),
        name="hidden",
    )(tp, own, *pieces, gate, up)


def result_kernel(a0, a1, a2, a3, d0, d1, d2, d3, out_ref):
    rows = a0.shape[0]
    res = dot(a0[...], d0[...])
    for a, d in ((a1, d1), (a2, d2), (a3, d3)):
        res = res + dot(a[...], d[...])
    shape = (rows // 8, 8, LANES)
    place = lax.broadcasted_iota(jnp.int32, shape, 1)
    last = res[:, BLOCKS * LANES :].reshape(shape)
    for b in range(BLOCKS):
        main = res[:, b * LANES : (b + 1) * LANES].reshape(shape)
        block = jnp.where(place < SLOTS, main, pltpu.roll(last, SLOTS - 2 * b, 1))
        out_ref[:, b * LANES : (b + 1) * LANES] = block.reshape(rows, LANES).astype(out_ref.dtype)


def results(acts, downs):
    rows = acts[0].shape[0]
    return pl.pallas_call(
        result_kernel,
        out_shape=jax.ShapeDtypeStruct((rows, BLOCKS * LANES), jnp.bfloat16),
        compiler_params=params(20),
        cost_estimate=cost(2 * rows * 1024 * 1024, 4 << 20),
        name="results",
    )(*acts, *downs)


def combine_kernel(chunk, target_ref, weight_ref, back_ref, *refs):
    out_ref = refs[-1]
    tokens = target_ref.shape[0]
    rows = back_ref.shape[0]
    lane = lax.broadcasted_iota(jnp.int32, (tokens, rows), 1)
    place = lane % 8
    first = (lane // 8) * 16 + chunk * SLOTS

    def mixing(slot):
        mix = jnp.zeros((tokens, rows), jnp.float32)
        for k in range(TOPK):
            mix = jnp.where(target_ref[:, k : k + 1] == slot, weight_ref[:, k : k + 1], mix)
        main = mix.astype(jnp.bfloat16)
        return main, (mix - main.astype(jnp.float32)).astype(jnp.bfloat16)

    main = mixing(jnp.where(place < SLOTS, first + place, -1))
    last = jnp.zeros((tokens, LANES), jnp.float32)
    for b in range(BLOCKS + 1):
        cols = slice(b * LANES, (b + 1) * LANES)
        if b < BLOCKS:
            block = back_ref[:, cols]
            extra = mixing(jnp.where(place < SLOTS, -1, first + 2 * b + place - SLOTS))
            last = last + dot(extra[0], block) + dot(extra[1], block)
            value = dot(main[0], block) + dot(main[1], block)
        else:
            value = last
        if len(refs) > 1:
            value = value + refs[0][:, cols]
        out_ref[:, cols] = value.astype(out_ref.dtype)


def combined(chunk, target, weight, back, *before):
    tokens = target.shape[0]
    dtype = jnp.bfloat16 if before else jnp.float32
    return pl.pallas_call(
        functools.partial(combine_kernel, chunk),
        out_shape=jax.ShapeDtypeStruct((tokens, (BLOCKS + 1) * LANES), dtype),
        compiler_params=params(12),
        cost_estimate=cost(10**9, 2 << 20),
        name="combine",
    )(target, weight, back, *before)


def program(
    projected_queries,
    key_proj,
    projected_values,
    head_sink_logits,
    out_weight,
    expert_input,
    norm_gain,
    routing,
    route_weight,
    gate_weight,
    up_weight,
    down_weight,
):
    bf = jnp.bfloat16
    tp = lax.axis_index("tp")
    at = tp.astype(jnp.int32).reshape(1)
    token_rows = expert_input.shape[0]
    experts = lax.axis_size("ep")
    share = D // N_TP

    ids = routing.T.reshape(-1)
    index = jnp.arange(ids.shape[0])
    same = (ids[:, None] == ids[None, :]) & (index[:, None] < index[None, :])
    rank = jnp.sum(same.astype(jnp.int32), axis=0)
    target = (ids * 16 + rank).reshape(TOPK, token_rows)

    widened = expert_input.astype(jnp.float32)
    scale = lax.rsqrt(jnp.mean(widened * widened, axis=-1, keepdims=True) + EPS)
    own = lax.dynamic_slice_in_dim(expert_input, tp * share, share, 1).astype(jnp.float32)
    gain = lax.dynamic_slice_in_dim(norm_gain, tp * share, share, 0)
    normed = (own * scale * gain[None, :]).astype(bf)

    got1 = exchanged(dispatched(0, target, normed, experts * 8))
    got2 = exchanged(dispatched(1, target, normed, experts * 8))

    downs = []
    for k in range(N_TP):
        block = lax.dynamic_slice_in_dim(down_weight[0], ((tp + N_TP - k) % N_TP) * share, share, 1)
        downs.append(shifted(block, k) if k else block)

    def activated(got):
        middle = got.shape[0] // 2
        top, bottom = got[:middle], got[middle:]
        nt, pt = shifted(top, 1), shifted(top, -1)
        nb, pb = shifted(bottom, 1), shifted(bottom, -1)
        ft, fb = shifted(nt, 1), shifted(pb, -1)
        return hidden(at, got, (nt, nb, ft, fb, pt, pb), gate_weight[0], up_weight[0])

    def spread(act):
        return (act, shifted(act, 1), shifted(act, 2), shifted(act, -1))

    back1 = exchanged(results(spread(activated(got1)), downs))
    back2 = exchanged(results(spread(activated(got2)), downs))

    attended = attention(projected_queries, key_proj, projected_values, head_sink_logits)
    partial = dot(attended, out_weight).astype(bf)
    owned = partial.shape[0] // N_TP
    mixed = None
    for k in range(N_TP):
        block = lax.dynamic_slice_in_dim(partial, ((tp + N_TP - k) % N_TP) * owned, owned, 0)
        block = (shifted(block, k) if k else block).astype(jnp.float32)
        mixed = block if mixed is None else mixed + block
    mixer_output = mixed.astype(bf)

    columns = target.T
    expert_output = combined(
        1, columns, route_weight, back2, combined(0, columns, route_weight, back1)
    )
    return (mixer_output, expert_output)


def solution(mesh):
    placed = (
        P("ep", "tp"),
        P("ep", "tp"),
        P("ep", "tp"),
        P("tp"),
        P("tp", None),
        P("ep", None),
        P(),
        P("ep", None),
        P("ep", None),
        P("ep", None, "tp"),
        P("ep", None, "tp"),
        P("ep", "tp", None),
    )
    return jax.shard_map(
        program,
        mesh=mesh,
        in_specs=placed,
        out_specs=(P(("ep", "tp"), None), P("ep", "tp")),
        check_vma=False,
    )
```

```python
import jax
import jax.numpy as jnp
from jax import lax
from jax.experimental import pallas as pl
from jax.experimental.pallas import tpu as pltpu
from jax.sharding import PartitionSpec as P

D = 4096
HEAD_SIZE = 64
WINDOW_KEYS = 128
TOPK = 4
EPS = 1e-06
CLAMP = 7.0
SLOPE = 1.702
N_TP = 4
SLOTS = 6
LANES = 256
BLOCKS = 3


def shifted(block, distance):
    return lax.ppermute(block, "tp", [((i + distance) % N_TP, i) for i in range(N_TP)])


def exchanged(block):
    return lax.all_to_all(block, "ep", split_axis=0, concat_axis=0, tiled=True)


def dot(a, b):
    return jnp.dot(a, b, preferred_element_type=jnp.float32)


def attention(projected_queries, key_proj, projected_values, head_sink_logits):
    query_rows = projected_queries.shape[0]
    kv_heads = key_proj.shape[1] // HEAD_SIZE
    heads_per_group = projected_queries.shape[1] // HEAD_SIZE // kv_heads
    count_of_blocks = query_rows // WINDOW_KEYS
    kept = key_proj.shape[1]
    prior = lax.ppermute(
        jnp.concatenate(
            [key_proj[query_rows - WINDOW_KEYS :], projected_values[query_rows - WINDOW_KEYS :]],
            axis=1,
        ),
        "ep",
        [(i, i + 1) for i in range(lax.axis_size("ep") - 1)],
    )
    prior_key, prior_value = prior[:, :kept], prior[:, kept:]
    key_all = jnp.concatenate([prior_key, key_proj], axis=0)
    value_all = jnp.concatenate([prior_value, projected_values], axis=0)
    window_keys = jnp.concatenate(
        [
            key_all[:-WINDOW_KEYS].reshape(count_of_blocks, WINDOW_KEYS, kv_heads, HEAD_SIZE),
            key_all[WINDOW_KEYS:].reshape(count_of_blocks, WINDOW_KEYS, kv_heads, HEAD_SIZE),
        ],
        axis=1,
    )
    window_values = jnp.concatenate(
        [
            value_all[:-WINDOW_KEYS].reshape(count_of_blocks, WINDOW_KEYS, kv_heads, HEAD_SIZE),
            value_all[WINDOW_KEYS:].reshape(count_of_blocks, WINDOW_KEYS, kv_heads, HEAD_SIZE),
        ],
        axis=1,
    )
    query_blocks = projected_queries.reshape(
        count_of_blocks, WINDOW_KEYS, kv_heads, heads_per_group, HEAD_SIZE
    )
    scores = jnp.einsum(
        "nqhgd,nshd->nhgqs", query_blocks, window_keys, preferred_element_type=jnp.float32
    ) * HEAD_SIZE ** (-0.5)
    offset = lax.axis_index("ep") * query_rows
    block_ids = jnp.arange(count_of_blocks)[:, None, None] * WINDOW_KEYS + offset
    query_pos = block_ids + jnp.arange(WINDOW_KEYS)[None, :, None]
    key_pos = block_ids - WINDOW_KEYS + jnp.arange(2 * WINDOW_KEYS)[None, None, :]
    permitted_mask = (key_pos <= query_pos) & (query_pos - key_pos < WINDOW_KEYS) & (key_pos >= 0)
    scores = jnp.where(permitted_mask[:, None, None, :, :], scores, -jnp.inf)
    sink_col = head_sink_logits.reshape(kv_heads, heads_per_group)[None, :, :, None, None]
    highest = jnp.maximum(jnp.max(scores, axis=-1, keepdims=True), sink_col)
    numerator = jnp.exp(scores - highest)
    denominator = jnp.sum(numerator, axis=-1, keepdims=True) + jnp.exp(sink_col - highest)
    weights = (numerator / denominator).astype(jnp.bfloat16)
    attended = jnp.einsum(
        "nhgqs,nshd->nqhgd", weights, window_values, preferred_element_type=jnp.float32
    )
    return attended.astype(jnp.bfloat16).reshape(
        query_rows, kv_heads * heads_per_group * HEAD_SIZE
    )


def params(mib):
    return pltpu.CompilerParams(vmem_limit_bytes=mib << 20)


def cost(flops, size):
    return pl.CostEstimate(flops=flops, bytes_accessed=size, transcendentals=0)


def dispatch_kernel(chunk_ref, target_ref, normed_ref, out_ref):
    rows = out_ref.shape[0]
    tokens = normed_ref.shape[0]
    row = lax.broadcasted_iota(jnp.int32, (rows, tokens), 0)
    place = row % 8
    first = (row // 8) * 16 + chunk_ref[0] * SLOTS

    def picks(slot):
        hit = target_ref[0:1, :] == slot
        for k in range(1, TOPK):
            hit = hit | (target_ref[k : k + 1, :] == slot)
        return jnp.where(hit, 1.0, 0.0).astype(jnp.bfloat16)

    main = picks(jnp.where(place < SLOTS, first + place, -1))
    last = normed_ref[:, BLOCKS * LANES :]
    for b in range(BLOCKS):
        extra = picks(jnp.where(place < SLOTS, -1, first + 2 * b + place - SLOTS))
        cols = slice(b * LANES, (b + 1) * LANES)
        out_ref[:, cols] = (dot(main, normed_ref[:, cols]) + dot(extra, last)).astype(out_ref.dtype)


def dispatched(chunk, target, normed, rows):
    vmem = pl.BlockSpec(memory_space=pltpu.VMEM)
    return pl.pallas_call(
        dispatch_kernel,
        in_specs=[pl.BlockSpec(memory_space=pltpu.SMEM), vmem, vmem],
        out_specs=vmem,
        out_shape=jax.ShapeDtypeStruct((rows, BLOCKS * LANES), jnp.bfloat16),
        compiler_params=params(12),
        cost_estimate=cost(4 * rows * 128 * 768, 1 << 20),
        name="dispatch",
    )(jnp.full((1,), chunk, jnp.int32), target, normed)


def hidden_kernel(tp_ref, own, nt, nb, ft, fb, pt, pb, gate_ref, up_ref, out_ref, held, acc, sems):
    step = pl.program_id(0)
    rows = own.shape[0]
    width = BLOCKS * LANES
    half = rows // 2
    copies = [pltpu.make_async_copy(own, held.at[0], sems.at[0])]
    for j, (top, bottom) in enumerate(((nt, nb), (ft, fb), (pt, pb))):
        for k, piece in enumerate((top, bottom)):
            copies.append(
                pltpu.make_async_copy(
                    piece, held.at[j + 1, pl.ds(k * half, half)], sems.at[1 + 2 * j + k]
                )
            )

    @pl.when(step == 0)
    def _():
        for copy in copies:
            copy.start()
        acc[...] = jnp.zeros(acc.shape, acc.dtype)
        copies[0].wait()

    for j in range(1, N_TP):

        @pl.when(step == j)
        def _():
            copies[2 * j - 1].wait()
            copies[2 * j].wait()

    shape = (rows // 8, 8, LANES)
    place = lax.broadcasted_iota(jnp.int32, shape, 1)
    moved = [
        pltpu.roll(
            held[step, :, b * LANES : (b + 1) * LANES].astype(jnp.float32).reshape(shape), 2 * b + 2, 1
        )
        for b in range(BLOCKS)
    ]
    last = jnp.where(place < 2, moved[0], jnp.where(place < 4, moved[1], moved[2]))
    last = last.reshape(rows, LANES).astype(jnp.bfloat16)
    for side, w_ref in enumerate((gate_ref, up_ref)):
        acc[side] += dot(held[step], w_ref[:width, :]) + dot(last, w_ref[width:, :])

    @pl.when(step == N_TP - 1)
    def _():
        gate_cut = jnp.minimum(acc[0], CLAMP)
        up_cut = jnp.clip(acc[1], -CLAMP, CLAMP)
        value = ((up_cut + 1.0) * gate_cut * jax.nn.sigmoid(SLOPE * gate_cut)).reshape(shape)
        count = rows // 32
        low = place[:count] < SLOTS
        fourth = value[BLOCKS * count :]
        for b in range(BLOCKS):
            packed = jnp.where(
                low, value[b * count : (b + 1) * count], pltpu.roll(fourth, SLOTS - 2 * b, 1)
            )
            out_ref[b * count * 8 : (b + 1) * count * 8, :] = packed.reshape(count * 8, LANES).astype(
                out_ref.dtype
            )


def hidden(tp, own, pieces, gate, up):
    rows, width = own.shape
    cols = gate.shape[1]
    weight = pl.BlockSpec((width + LANES, cols), lambda j, t: ((t[0] + j) % N_TP, 0))
    return pl.pallas_call(
        hidden_kernel,
        grid_spec=pltpu.PrefetchScalarGridSpec(
            num_scalar_prefetch=1,
            grid=(N_TP,),
            in_specs=[pl.BlockSpec(memory_space=pl.ANY)] * 7 + [weight] * 2,
            out_specs=pl.BlockSpec((rows * 3 // 4, cols), lambda j, t: (0, 0)),
            scratch_shapes=[
                pltpu.VMEM((N_TP, rows, width), jnp.bfloat16),
                pltpu.VMEM((2, rows, cols), jnp.float32),
                pltpu.SemaphoreType.DMA((7,)),
            ],
        ),
        out_shape=jax.ShapeDtypeStruct((rows * 3 // 4, cols), jnp.bfloat16),
        compiler_params=params(56),
        cost_estimate=cost(8 * rows * width * cols, 8 << 20),
        name="hidden",
    )(tp, own, *pieces, gate, up)


def result_kernel(a0, a1, a2, a3, d0, d1, d2, d3, out_ref):
    res = dot(a0[...], d0[...])
    for a, d in ((a1, d1), (a2, d2), (a3, d3)):
        res = res + dot(a[...], d[...])
    count = res.shape[0] // 24
    shape = (BLOCKS * count, 8, LANES)
    place = lax.broadcasted_iota(jnp.int32, (count, 8, LANES), 1)

    def unpacked(cols):
        value = res[:, cols].reshape(shape)
        parts = [value[b * count : (b + 1) * count] for b in range(BLOCKS)]
        moved = [pltpu.roll(part, 2 * b + 2, 1) for b, part in enumerate(parts)]
        return parts + [jnp.where(place < 2, moved[0], jnp.where(place < 4, moved[1], moved[2]))]

    last = unpacked(slice(BLOCKS * LANES, (BLOCKS + 1) * LANES))
    for b in range(BLOCKS):
        main = unpacked(slice(b * LANES, (b + 1) * LANES))
        for q in range(4):
            block = jnp.where(place < SLOTS, main[q], pltpu.roll(last[q], SLOTS - 2 * b, 1))
            out_ref[q * count * 8 : (q + 1) * count * 8, b * LANES : (b + 1) * LANES] = block.reshape(
                count * 8, LANES
            ).astype(out_ref.dtype)


def results(acts, downs):
    rows = acts[0].shape[0]
    return pl.pallas_call(
        result_kernel,
        out_shape=jax.ShapeDtypeStruct((rows * 4 // 3, BLOCKS * LANES), jnp.bfloat16),
        compiler_params=params(14),
        cost_estimate=cost(2 * rows * 1024 * 1024, 4 << 20),
        name="results",
    )(*acts, *downs)


def combine_kernel(chunk_ref, target_ref, weight_ref, back_ref, before_ref, sum_ref, out_ref):
    tokens = target_ref.shape[0]
    rows = back_ref.shape[0]
    lane = lax.broadcasted_iota(jnp.int32, (tokens, rows), 1)
    place = lane % 8
    first = (lane // 8) * 16 + chunk_ref[0] * SLOTS

    def mixing(slot):
        mix = jnp.zeros((tokens, rows), jnp.float32)
        for k in range(TOPK):
            mix = jnp.where(target_ref[:, k : k + 1] == slot, weight_ref[:, k : k + 1], mix)
        main = mix.astype(jnp.bfloat16)
        return main, (mix - main.astype(jnp.float32)).astype(jnp.bfloat16)

    main = mixing(jnp.where(place < SLOTS, first + place, -1))
    last = jnp.zeros((tokens, LANES), jnp.float32)
    for b in range(BLOCKS + 1):
        cols = slice(b * LANES, (b + 1) * LANES)
        if b < BLOCKS:
            block = back_ref[:, cols]
            extra = mixing(jnp.where(place < SLOTS, -1, first + 2 * b + place - SLOTS))
            last = last + dot(extra[0], block) + dot(extra[1], block)
            value = dot(main[0], block) + dot(main[1], block)
        else:
            value = last
        value = value + before_ref[:, cols]
        sum_ref[:, cols] = value
        out_ref[:, cols] = value.astype(out_ref.dtype)


def combined(chunk, target, weight, back, before):
    vmem = pl.BlockSpec(memory_space=pltpu.VMEM)
    return pl.pallas_call(
        combine_kernel,
        in_specs=[pl.BlockSpec(memory_space=pltpu.SMEM)] + [vmem] * 4,
        out_specs=[vmem] * 2,
        out_shape=[
            jax.ShapeDtypeStruct(before.shape, jnp.float32),
            jax.ShapeDtypeStruct(before.shape, jnp.bfloat16),
        ],
        compiler_params=params(12),
        cost_estimate=cost(10**9, 2 << 20),
        name="combine",
    )(jnp.full((1,), chunk, jnp.int32), target, weight, back, before)


def program(
    projected_queries,
    key_proj,
    projected_values,
    head_sink_logits,
    out_weight,
    expert_input,
    norm_gain,
    routing,
    route_weight,
    gate_weight,
    up_weight,
    down_weight,
):
    bf = jnp.bfloat16
    tp = lax.axis_index("tp")
    at = tp.astype(jnp.int32).reshape(1)
    token_rows = expert_input.shape[0]
    experts = lax.axis_size("ep")
    share = D // N_TP

    ids = routing.T.reshape(-1)
    index = jnp.arange(ids.shape[0])
    same = (ids[:, None] == ids[None, :]) & (index[:, None] < index[None, :])
    rank = jnp.sum(same.astype(jnp.int32), axis=0)
    target = (ids * 16 + rank).reshape(TOPK, token_rows)

    widened = expert_input.astype(jnp.float32)
    scale = lax.rsqrt(jnp.mean(widened * widened, axis=-1, keepdims=True) + EPS)
    own = lax.dynamic_slice_in_dim(expert_input, tp * share, share, 1).astype(jnp.float32)
    gain = lax.dynamic_slice_in_dim(norm_gain, tp * share, share, 0)
    normed = (own * scale * gain[None, :]).astype(bf)

    got1 = exchanged(dispatched(0, target, normed, experts * 8))
    got2 = exchanged(dispatched(1, target, normed, experts * 8))

    downs = []
    for k in range(N_TP):
        block = lax.dynamic_slice_in_dim(down_weight[0], ((tp + N_TP - k) % N_TP) * share, share, 1)
        downs.append(shifted(block, k) if k else block)

    def activated(got):
        middle = got.shape[0] // 2
        top, bottom = got[:middle], got[middle:]
        nt, pt = shifted(top, 1), shifted(top, -1)
        nb, pb = shifted(bottom, 1), shifted(bottom, -1)
        ft, fb = shifted(nt, 1), shifted(pb, -1)
        return hidden(at, got, (nt, nb, ft, fb, pt, pb), gate_weight[0], up_weight[0])

    def spread(act):
        return (act, shifted(act, 1), shifted(act, 2), shifted(act, -1))

    back1 = exchanged(results(spread(activated(got1)), downs))
    back2 = exchanged(results(spread(activated(got2)), downs))

    attended = attention(projected_queries, key_proj, projected_values, head_sink_logits)
    partial = dot(attended, out_weight).astype(bf)
    owned = partial.shape[0] // N_TP
    mixed = None
    for k in range(N_TP):
        block = lax.dynamic_slice_in_dim(partial, ((tp + N_TP - k) % N_TP) * owned, owned, 0)
        block = (shifted(block, k) if k else block).astype(jnp.float32)
        mixed = block if mixed is None else mixed + block
    mixer_output = mixed.astype(bf)

    columns = target.T
    start = jnp.zeros((token_rows, share), jnp.float32)
    so_far = combined(0, columns, route_weight, back1, start)[0]
    expert_output = combined(1, columns, route_weight, back2, so_far)[1]
    return (mixer_output, expert_output)


def solution(mesh):
    placed = (
        P("ep", "tp"),
        P("ep", "tp"),
        P("ep", "tp"),
        P("tp"),
        P("tp", None),
        P("ep", None),
        P(),
        P("ep", None),
        P("ep", None),
        P("ep", None, "tp"),
        P("ep", None, "tp"),
        P("ep", "tp", None),
    )
    return jax.shard_map(
        program,
        mesh=mesh,
        in_specs=placed,
        out_specs=(P(("ep", "tp"), None), P("ep", "tp")),
        check_vma=False,
    )
```

```python
import jax
import jax.numpy as jnp
from jax import lax
from jax.experimental import pallas as pl
from jax.experimental.pallas import tpu as pltpu
from jax.sharding import PartitionSpec as P

D = 4096
HEAD_SIZE = 64
WINDOW_KEYS = 128
TOPK = 4
EPS = 1e-06
CLAMP = 7.0
SLOPE = 1.702
N_TP = 4
SLOTS = 6
LANES = 256
BLOCKS = 3


def shifted(block, distance):
    return lax.ppermute(block, "tp", [((i + distance) % N_TP, i) for i in range(N_TP)])


def exchanged(block):
    return lax.all_to_all(block, "ep", split_axis=0, concat_axis=0, tiled=True)


def dot(a, b):
    return jnp.dot(a, b, preferred_element_type=jnp.float32)


def params(mib):
    return pltpu.CompilerParams(vmem_limit_bytes=mib << 20)


def cost(flops, size):
    return pl.CostEstimate(flops=flops, bytes_accessed=size, transcendentals=0)


def dispatch_kernel(chunk_ref, target_ref, normed_ref, out_ref):
    rows = out_ref.shape[0]
    tokens = normed_ref.shape[0]
    row = lax.broadcasted_iota(jnp.int32, (rows, tokens), 0)
    place = row % 8
    first = (row // 8) * 16 + chunk_ref[0] * SLOTS

    def picks(slot):
        hit = target_ref[0:1, :] == slot
        for k in range(1, TOPK):
            hit = hit | (target_ref[k : k + 1, :] == slot)
        return jnp.where(hit, 1.0, 0.0).astype(jnp.bfloat16)

    main = picks(jnp.where(place < SLOTS, first + place, -1))
    last = normed_ref[:, BLOCKS * LANES :]
    for b in range(BLOCKS):
        extra = picks(jnp.where(place < SLOTS, -1, first + 2 * b + place - SLOTS))
        cols = slice(b * LANES, (b + 1) * LANES)
        out_ref[:, cols] = (dot(main, normed_ref[:, cols]) + dot(extra, last)).astype(out_ref.dtype)


def dispatched(chunk, target, normed, rows):
    vmem = pl.BlockSpec(memory_space=pltpu.VMEM)
    return pl.pallas_call(
        dispatch_kernel,
        in_specs=[pl.BlockSpec(memory_space=pltpu.SMEM), vmem, vmem],
        out_specs=vmem,
        out_shape=jax.ShapeDtypeStruct((rows, BLOCKS * LANES), jnp.bfloat16),
        compiler_params=params(12),
        cost_estimate=cost(4 * rows * 128 * 768, 1 << 20),
        name="dispatch",
    )(jnp.full((1,), chunk, jnp.int32), target, normed)


def hidden_kernel(tp_ref, own, nt, nb, ft, fb, pt, pb, gate_ref, up_ref, out_ref, held, acc, sems):
    step = pl.program_id(0)
    rows = own.shape[0]
    width = BLOCKS * LANES
    half = rows // 2
    copies = [pltpu.make_async_copy(own, held.at[0], sems.at[0])]
    for j, (top, bottom) in enumerate(((nt, nb), (ft, fb), (pt, pb))):
        for k, piece in enumerate((top, bottom)):
            copies.append(
                pltpu.make_async_copy(
                    piece, held.at[j + 1, pl.ds(k * half, half)], sems.at[1 + 2 * j + k]
                )
            )

    @pl.when(step == 0)
    def _():
        for copy in copies:
            copy.start()
        acc[...] = jnp.zeros(acc.shape, acc.dtype)
        copies[0].wait()

    for j in range(1, N_TP):

        @pl.when(step == j)
        def _():
            copies[2 * j - 1].wait()
            copies[2 * j].wait()

    shape = (rows // 8, 8, LANES)
    place = lax.broadcasted_iota(jnp.int32, shape, 1)
    moved = [
        pltpu.roll(
            held[step, :, b * LANES : (b + 1) * LANES].astype(jnp.float32).reshape(shape), 2 * b + 2, 1
        )
        for b in range(BLOCKS)
    ]
    last = jnp.where(place < 2, moved[0], jnp.where(place < 4, moved[1], moved[2]))
    last = last.reshape(rows, LANES).astype(jnp.bfloat16)
    for side, w_ref in enumerate((gate_ref, up_ref)):
        acc[side] += dot(held[step], w_ref[:width, :]) + dot(last, w_ref[width:, :])

    @pl.when(step == N_TP - 1)
    def _():
        gate_cut = jnp.minimum(acc[0], CLAMP)
        up_cut = jnp.clip(acc[1], -CLAMP, CLAMP)
        value = ((up_cut + 1.0) * gate_cut * jax.nn.sigmoid(SLOPE * gate_cut)).reshape(shape)
        count = rows // 32
        low = place[:count] < SLOTS
        fourth = value[BLOCKS * count :]
        for b in range(BLOCKS):
            packed = jnp.where(
                low, value[b * count : (b + 1) * count], pltpu.roll(fourth, SLOTS - 2 * b, 1)
            )
            out_ref[b * count * 8 : (b + 1) * count * 8, :] = packed.reshape(count * 8, LANES).astype(
                out_ref.dtype
            )


def hidden(tp, own, pieces, gate, up):
    rows, width = own.shape
    cols = gate.shape[1]
    weight = pl.BlockSpec((width + LANES, cols), lambda j, t: ((t[0] + j) % N_TP, 0))
    return pl.pallas_call(
        hidden_kernel,
        grid_spec=pltpu.PrefetchScalarGridSpec(
            num_scalar_prefetch=1,
            grid=(N_TP,),
            in_specs=[pl.BlockSpec(memory_space=pl.ANY)] * 7 + [weight] * 2,
            out_specs=pl.BlockSpec((rows * 3 // 4, cols), lambda j, t: (0, 0)),
            scratch_shapes=[
                pltpu.VMEM((N_TP, rows, width), jnp.bfloat16),
                pltpu.VMEM((2, rows, cols), jnp.float32),
                pltpu.SemaphoreType.DMA((7,)),
            ],
        ),
        out_shape=jax.ShapeDtypeStruct((rows * 3 // 4, cols), jnp.bfloat16),
        compiler_params=params(56),
        cost_estimate=cost(8 * rows * width * cols, 8 << 20),
        name="hidden",
    )(tp, own, *pieces, gate, up)


def result_kernel(a0, a1, a2, a3, d0, d1, d2, d3, out_ref):
    res = dot(a0[...], d0[...])
    for a, d in ((a1, d1), (a2, d2), (a3, d3)):
        res = res + dot(a[...], d[...])
    count = res.shape[0] // 24
    shape = (BLOCKS * count, 8, LANES)
    place = lax.broadcasted_iota(jnp.int32, (count, 8, LANES), 1)

    def unpacked(cols):
        value = res[:, cols].reshape(shape)
        parts = [value[b * count : (b + 1) * count] for b in range(BLOCKS)]
        moved = [pltpu.roll(part, 2 * b + 2, 1) for b, part in enumerate(parts)]
        return parts + [jnp.where(place < 2, moved[0], jnp.where(place < 4, moved[1], moved[2]))]

    last = unpacked(slice(BLOCKS * LANES, (BLOCKS + 1) * LANES))
    for b in range(BLOCKS):
        main = unpacked(slice(b * LANES, (b + 1) * LANES))
        for q in range(4):
            block = jnp.where(place < SLOTS, main[q], pltpu.roll(last[q], SLOTS - 2 * b, 1))
            out_ref[q * count * 8 : (q + 1) * count * 8, b * LANES : (b + 1) * LANES] = block.reshape(
                count * 8, LANES
            ).astype(out_ref.dtype)


def results(acts, downs):
    rows = acts[0].shape[0]
    return pl.pallas_call(
        result_kernel,
        out_shape=jax.ShapeDtypeStruct((rows * 4 // 3, BLOCKS * LANES), jnp.bfloat16),
        compiler_params=params(14),
        cost_estimate=cost(2 * rows * 1024 * 1024, 4 << 20),
        name="results",
    )(*acts, *downs)


def attention_kernel(ep_ref, sink_ref, q_ref, k_ref, v_ref, prior_ref, out_ref):
    block = WINDOW_KEYS
    tiles = q_ref.shape[1] // 128
    query = lax.broadcasted_iota(jnp.int32, (block, 2 * block), 0)
    key = lax.broadcasted_iota(jnp.int32, (block, 2 * block), 1)
    lane = lax.broadcasted_iota(jnp.int32, (block, 128), 1)
    for n in range(q_ref.shape[0] // block):
        own = slice(n * block, (n + 1) * block)
        before = slice((n - 1) * block, n * block)
        allowed = (key > query) & (key <= query + block)
        if n == 0:
            allowed = allowed & (key >= jnp.where(ep_ref[0] == 0, block, 0))
            key_prior, value_prior = prior_ref[:, :128], prior_ref[:, 128:]
        else:
            key_prior, value_prior = k_ref[before, :], v_ref[before, :]
        keys = jnp.concatenate([key_prior, k_ref[own, :]], axis=0)
        values = jnp.concatenate([value_prior, v_ref[own, :]], axis=0)
        for t in range(tiles):
            tile = q_ref[own, t * 128 : (t + 1) * 128].astype(jnp.float32)
            group = t // 2
            parts = []
            for e in range(2):
                head = tile if e == group else pltpu.roll(tile, HEAD_SIZE, 1)
                head = jnp.where(lane // HEAD_SIZE == group, head, 0.0).astype(jnp.bfloat16)
                scores = lax.dot_general(
                    head, keys, (((1,), (1,)), ((), ())), preferred_element_type=jnp.float32
                ) * HEAD_SIZE ** (-0.5)
                scores = jnp.where(allowed, scores, -jnp.inf)
                sink = sink_ref[2 * t + e]
                highest = jnp.maximum(jnp.max(scores, axis=1, keepdims=True), sink)
                numerator = jnp.exp(scores - highest)
                denominator = jnp.sum(numerator, axis=1, keepdims=True) + jnp.exp(sink - highest)
                weights = (numerator * (1.0 / denominator)).astype(jnp.bfloat16)
                result = dot(weights, values)
                parts.append(result if e == group else pltpu.roll(result, HEAD_SIZE, 1))
            out_ref[own, t * 128 : (t + 1) * 128] = jnp.where(
                lane < HEAD_SIZE, parts[0], parts[1]
            ).astype(out_ref.dtype)


def attention(queries, keys, values, sinks):
    rows = queries.shape[0]
    last = [x[rows - WINDOW_KEYS :] for x in (keys, values)]
    prior = lax.ppermute(
        jnp.concatenate(last, axis=1), "ep", [(i, i + 1) for i in range(lax.axis_size("ep") - 1)]
    )
    vmem = pl.BlockSpec(memory_space=pltpu.VMEM)
    smem = pl.BlockSpec(memory_space=pltpu.SMEM)
    return pl.pallas_call(
        attention_kernel,
        in_specs=[smem, smem] + [vmem] * 4,
        out_specs=vmem,
        out_shape=jax.ShapeDtypeStruct(queries.shape, jnp.bfloat16),
        compiler_params=params(12),
        cost_estimate=cost(10**9, 1 << 20),
        name="attention",
    )(lax.axis_index("ep").astype(jnp.int32).reshape(1), sinks, queries, keys, values, prior)


def combine_kernel(chunk_ref, target_ref, weight_ref, back_ref, before_ref, sum_ref, out_ref):
    tokens = target_ref.shape[0]
    rows = back_ref.shape[0]
    lane = lax.broadcasted_iota(jnp.int32, (tokens, rows), 1)
    place = lane % 8
    first = (lane // 8) * 16 + chunk_ref[0] * SLOTS

    def mixing(slot):
        mix = jnp.zeros((tokens, rows), jnp.float32)
        for k in range(TOPK):
            mix = jnp.where(target_ref[:, k : k + 1] == slot, weight_ref[:, k : k + 1], mix)
        main = mix.astype(jnp.bfloat16)
        return main, (mix - main.astype(jnp.float32)).astype(jnp.bfloat16)

    main = mixing(jnp.where(place < SLOTS, first + place, -1))
    last = jnp.zeros((tokens, LANES), jnp.float32)
    for b in range(BLOCKS + 1):
        cols = slice(b * LANES, (b + 1) * LANES)
        if b < BLOCKS:
            block = back_ref[:, cols]
            extra = mixing(jnp.where(place < SLOTS, -1, first + 2 * b + place - SLOTS))
            last = last + dot(extra[0], block) + dot(extra[1], block)
            value = dot(main[0], block) + dot(main[1], block)
        else:
            value = last
        value = value + before_ref[:, cols]
        sum_ref[:, cols] = value
        out_ref[:, cols] = value.astype(out_ref.dtype)


def combined(chunk, target, weight, back, before):
    vmem = pl.BlockSpec(memory_space=pltpu.VMEM)
    return pl.pallas_call(
        combine_kernel,
        in_specs=[pl.BlockSpec(memory_space=pltpu.SMEM)] + [vmem] * 4,
        out_specs=[vmem] * 2,
        out_shape=[
            jax.ShapeDtypeStruct(before.shape, jnp.float32),
            jax.ShapeDtypeStruct(before.shape, jnp.bfloat16),
        ],
        compiler_params=params(12),
        cost_estimate=cost(10**9, 2 << 20),
        name="combine",
    )(jnp.full((1,), chunk, jnp.int32), target, weight, back, before)


def program(
    projected_queries,
    key_proj,
    projected_values,
    head_sink_logits,
    out_weight,
    expert_input,
    norm_gain,
    routing,
    route_weight,
    gate_weight,
    up_weight,
    down_weight,
):
    bf = jnp.bfloat16
    tp = lax.axis_index("tp")
    at = tp.astype(jnp.int32).reshape(1)
    token_rows = expert_input.shape[0]
    experts = lax.axis_size("ep")
    share = D // N_TP

    ids = routing.T.reshape(-1)
    index = jnp.arange(ids.shape[0])
    same = (ids[:, None] == ids[None, :]) & (index[:, None] < index[None, :])
    rank = jnp.sum(same.astype(jnp.int32), axis=0)
    target = (ids * 16 + rank).reshape(TOPK, token_rows)

    widened = expert_input.astype(jnp.float32)
    scale = lax.rsqrt(jnp.mean(widened * widened, axis=-1, keepdims=True) + EPS)
    own = lax.dynamic_slice_in_dim(expert_input, tp * share, share, 1).astype(jnp.float32)
    gain = lax.dynamic_slice_in_dim(norm_gain, tp * share, share, 0)
    normed = (own * scale * gain[None, :]).astype(bf)

    got1 = exchanged(dispatched(0, target, normed, experts * 8))
    got2 = exchanged(dispatched(1, target, normed, experts * 8))

    downs = []
    for k in range(N_TP):
        block = lax.dynamic_slice_in_dim(down_weight[0], ((tp + N_TP - k) % N_TP) * share, share, 1)
        downs.append(shifted(block, k) if k else block)

    def activated(got):
        middle = got.shape[0] // 2
        top, bottom = got[:middle], got[middle:]
        nt, pt = shifted(top, 1), shifted(top, -1)
        nb, pb = shifted(bottom, 1), shifted(bottom, -1)
        ft, fb = shifted(nt, 1), shifted(pb, -1)
        return hidden(at, got, (nt, nb, ft, fb, pt, pb), gate_weight[0], up_weight[0])

    def spread(act):
        return (act, shifted(act, 1), shifted(act, 2), shifted(act, -1))

    back1 = exchanged(results(spread(activated(got1)), downs))
    back2 = exchanged(results(spread(activated(got2)), downs))

    attended = attention(projected_queries, key_proj, projected_values, head_sink_logits)
    partial = dot(attended, out_weight).astype(bf)
    owned = partial.shape[0] // N_TP
    mixed = None
    for k in range(N_TP):
        block = lax.dynamic_slice_in_dim(partial, ((tp + N_TP - k) % N_TP) * owned, owned, 0)
        block = (shifted(block, k) if k else block).astype(jnp.float32)
        mixed = block if mixed is None else mixed + block
    mixer_output = mixed.astype(bf)

    columns = target.T
    start = jnp.zeros((token_rows, share), jnp.float32)
    so_far = combined(0, columns, route_weight, back1, start)[0]
    expert_output = combined(1, columns, route_weight, back2, so_far)[1]
    return (mixer_output, expert_output)


def solution(mesh):
    placed = (
        P("ep", "tp"),
        P("ep", "tp"),
        P("ep", "tp"),
        P("tp"),
        P("tp", None),
        P("ep", None),
        P(),
        P("ep", None),
        P("ep", None),
        P("ep", None, "tp"),
        P("ep", None, "tp"),
        P("ep", "tp", None),
    )
    return jax.shard_map(
        program,
        mesh=mesh,
        in_specs=placed,
        out_specs=(P(("ep", "tp"), None), P("ep", "tp")),
        check_vma=False,
    )
```

```python
import jax
import jax.numpy as jnp
from jax import lax
from jax.experimental import pallas as pl
from jax.experimental.pallas import tpu as pltpu
from jax.sharding import PartitionSpec as P

D = 4096
HEAD_SIZE = 64
WINDOW_KEYS = 128
TOPK = 4
EPS = 1e-06
CLAMP = 7.0
SLOPE = 1.702
N_TP = 4
SLOTS = 6
LANES = 256
BLOCKS = 3


def shifted(block, distance):
    return lax.ppermute(block, "tp", [((i + distance) % N_TP, i) for i in range(N_TP)])


def exchanged(block):
    return lax.all_to_all(block, "ep", split_axis=0, concat_axis=0, tiled=True)


def dot(a, b):
    return jnp.dot(a, b, preferred_element_type=jnp.float32)


def params(mib):
    return pltpu.CompilerParams(vmem_limit_bytes=mib << 20)


def cost(flops, size):
    return pl.CostEstimate(flops=flops, bytes_accessed=size, transcendentals=0)


def dispatch_kernel(at_ref, target_ref, input_ref, gain_ref, out_ref):
    rows = out_ref.shape[0]
    tokens, features = input_ref.shape
    share = features // N_TP
    own = pl.ds(pl.multiple_of(at_ref[1] * share, share), share)
    squares = jnp.zeros((tokens, share), jnp.float32)
    for k in range(N_TP):
        part = input_ref[:, k * share : (k + 1) * share].astype(jnp.float32)
        squares = squares + part * part
    scale = lax.rsqrt(jnp.sum(squares, axis=1, keepdims=True) * (1.0 / features) + EPS)
    normed = (input_ref[:, own].astype(jnp.float32) * scale * gain_ref[:, own]).astype(jnp.bfloat16)
    row = lax.broadcasted_iota(jnp.int32, (rows, tokens), 0)
    place = row % 8
    first = (row // 8) * 16 + at_ref[0] * SLOTS

    def picks(slot):
        hit = target_ref[0:1, :] == slot
        for k in range(1, TOPK):
            hit = hit | (target_ref[k : k + 1, :] == slot)
        return jnp.where(hit, 1.0, 0.0).astype(jnp.bfloat16)

    main = picks(jnp.where(place < SLOTS, first + place, -1))
    last = normed[:, BLOCKS * LANES :]
    for b in range(BLOCKS):
        extra = picks(jnp.where(place < SLOTS, -1, first + 2 * b + place - SLOTS))
        cols = slice(b * LANES, (b + 1) * LANES)
        out_ref[:, cols] = (dot(main, normed[:, cols]) + dot(extra, last)).astype(out_ref.dtype)


def dispatched(chunk, tp, target, tokens, gain, rows):
    vmem = pl.BlockSpec(memory_space=pltpu.VMEM)
    return pl.pallas_call(
        dispatch_kernel,
        in_specs=[pl.BlockSpec(memory_space=pltpu.SMEM), vmem, vmem, vmem],
        out_specs=vmem,
        out_shape=jax.ShapeDtypeStruct((rows, BLOCKS * LANES), jnp.bfloat16),
        compiler_params=params(56),
        cost_estimate=cost(4 * rows * 128 * 768, 1 << 20),
        name="dispatch",
    )(jnp.stack([jnp.int32(chunk), tp]), target, tokens, gain)


def hidden_kernel(tp_ref, own, nt, nb, ft, fb, pt, pb, gate_ref, up_ref, out_ref, held, acc, sems):
    step = pl.program_id(0)
    rows = own.shape[0]
    width = BLOCKS * LANES
    half = rows // 2
    copies = [pltpu.make_async_copy(own, held.at[0], sems.at[0])]
    for j, (top, bottom) in enumerate(((nt, nb), (ft, fb), (pt, pb))):
        for k, piece in enumerate((top, bottom)):
            copies.append(
                pltpu.make_async_copy(
                    piece, held.at[j + 1, pl.ds(k * half, half)], sems.at[1 + 2 * j + k]
                )
            )

    @pl.when(step == 0)
    def _():
        for copy in copies:
            copy.start()
        acc[...] = jnp.zeros(acc.shape, acc.dtype)
        copies[0].wait()

    for j in range(1, N_TP):

        @pl.when(step == j)
        def _():
            copies[2 * j - 1].wait()
            copies[2 * j].wait()

    shape = (rows // 8, 8, LANES)
    place = lax.broadcasted_iota(jnp.int32, shape, 1)
    moved = [
        pltpu.roll(
            held[step, :, b * LANES : (b + 1) * LANES].astype(jnp.float32).reshape(shape), 2 * b + 2, 1
        )
        for b in range(BLOCKS)
    ]
    last = jnp.where(place < 2, moved[0], jnp.where(place < 4, moved[1], moved[2]))
    last = last.reshape(rows, LANES).astype(jnp.bfloat16)
    for side, w_ref in enumerate((gate_ref, up_ref)):
        acc[side] += dot(held[step], w_ref[:width, :]) + dot(last, w_ref[width:, :])

    @pl.when(step == N_TP - 1)
    def _():
        gate_cut = jnp.minimum(acc[0], CLAMP)
        up_cut = jnp.clip(acc[1], -CLAMP, CLAMP)
        value = ((up_cut + 1.0) * gate_cut * jax.nn.sigmoid(SLOPE * gate_cut)).reshape(shape)
        count = rows // 32
        low = place[:count] < SLOTS
        fourth = value[BLOCKS * count :]
        for b in range(BLOCKS):
            packed = jnp.where(
                low, value[b * count : (b + 1) * count], pltpu.roll(fourth, SLOTS - 2 * b, 1)
            )
            out_ref[b * count * 8 : (b + 1) * count * 8, :] = packed.reshape(count * 8, LANES).astype(
                out_ref.dtype
            )


def hidden(tp, own, pieces, gate, up):
    rows, width = own.shape
    cols = gate.shape[1]
    weight = pl.BlockSpec((width + LANES, cols), lambda j, t: ((t[0] + j) % N_TP, 0))
    return pl.pallas_call(
        hidden_kernel,
        grid_spec=pltpu.PrefetchScalarGridSpec(
            num_scalar_prefetch=1,
            grid=(N_TP,),
            in_specs=[pl.BlockSpec(memory_space=pl.ANY)] * 7 + [weight] * 2,
            out_specs=pl.BlockSpec((rows * 3 // 4, cols), lambda j, t: (0, 0)),
            scratch_shapes=[
                pltpu.VMEM((N_TP, rows, width), jnp.bfloat16),
                pltpu.VMEM((2, rows, cols), jnp.float32),
                pltpu.SemaphoreType.DMA((7,)),
            ],
        ),
        out_shape=jax.ShapeDtypeStruct((rows * 3 // 4, cols), jnp.bfloat16),
        compiler_params=params(56),
        cost_estimate=cost(8 * rows * width * cols, 8 << 20),
        name="hidden",
    )(tp, own, *pieces, gate, up)


def result_kernel(a0, a1, a2, a3, d0, d1, d2, d3, out_ref):
    res = dot(a0[...], d0[...])
    for a, d in ((a1, d1), (a2, d2), (a3, d3)):
        res = res + dot(a[...], d[...])
    count = res.shape[0] // 24
    shape = (BLOCKS * count, 8, LANES)
    place = lax.broadcasted_iota(jnp.int32, (count, 8, LANES), 1)

    def unpacked(cols):
        value = res[:, cols].reshape(shape)
        parts = [value[b * count : (b + 1) * count] for b in range(BLOCKS)]
        moved = [pltpu.roll(part, 2 * b + 2, 1) for b, part in enumerate(parts)]
        return parts + [jnp.where(place < 2, moved[0], jnp.where(place < 4, moved[1], moved[2]))]

    last = unpacked(slice(BLOCKS * LANES, (BLOCKS + 1) * LANES))
    for b in range(BLOCKS):
        main = unpacked(slice(b * LANES, (b + 1) * LANES))
        for q in range(4):
            block = jnp.where(place < SLOTS, main[q], pltpu.roll(last[q], SLOTS - 2 * b, 1))
            out_ref[q * count * 8 : (q + 1) * count * 8, b * LANES : (b + 1) * LANES] = block.reshape(
                count * 8, LANES
            ).astype(out_ref.dtype)


def results(acts, downs):
    rows = acts[0].shape[0]
    return pl.pallas_call(
        result_kernel,
        out_shape=jax.ShapeDtypeStruct((rows * 4 // 3, BLOCKS * LANES), jnp.bfloat16),
        compiler_params=params(14),
        cost_estimate=cost(2 * rows * 1024 * 1024, 4 << 20),
        name="results",
    )(*acts, *downs)


def attention_kernel(ep_ref, sink_ref, q_ref, k_ref, v_ref, prior_ref, out_ref):
    block = WINDOW_KEYS
    tiles = q_ref.shape[1] // 128
    query = lax.broadcasted_iota(jnp.int32, (block, 2 * block), 0)
    key = lax.broadcasted_iota(jnp.int32, (block, 2 * block), 1)
    lane = lax.broadcasted_iota(jnp.int32, (block, 128), 1)
    for n in range(q_ref.shape[0] // block):
        own = slice(n * block, (n + 1) * block)
        before = slice((n - 1) * block, n * block)
        allowed = (key > query) & (key <= query + block)
        if n == 0:
            allowed = allowed & (key >= jnp.where(ep_ref[0] == 0, block, 0))
            key_prior, value_prior = prior_ref[:, :128], prior_ref[:, 128:]
        else:
            key_prior, value_prior = k_ref[before, :], v_ref[before, :]
        keys = jnp.concatenate([key_prior, k_ref[own, :]], axis=0)
        values = jnp.concatenate([value_prior, v_ref[own, :]], axis=0)
        for t in range(tiles):
            tile = q_ref[own, t * 128 : (t + 1) * 128].astype(jnp.float32)
            group = t // 2
            parts = []
            for e in range(2):
                head = tile if e == group else pltpu.roll(tile, HEAD_SIZE, 1)
                head = jnp.where(lane // HEAD_SIZE == group, head, 0.0).astype(jnp.bfloat16)
                scores = lax.dot_general(
                    head, keys, (((1,), (1,)), ((), ())), preferred_element_type=jnp.float32
                ) * HEAD_SIZE ** (-0.5)
                scores = jnp.where(allowed, scores, -jnp.inf)
                sink = sink_ref[2 * t + e]
                highest = jnp.maximum(jnp.max(scores, axis=1, keepdims=True), sink)
                numerator = jnp.exp(scores - highest)
                denominator = jnp.sum(numerator, axis=1, keepdims=True) + jnp.exp(sink - highest)
                weights = (numerator * (1.0 / denominator)).astype(jnp.bfloat16)
                result = dot(weights, values)
                parts.append(result if e == group else pltpu.roll(result, HEAD_SIZE, 1))
            out_ref[own, t * 128 : (t + 1) * 128] = jnp.where(
                lane < HEAD_SIZE, parts[0], parts[1]
            ).astype(out_ref.dtype)


def attention(queries, keys, values, sinks):
    rows = queries.shape[0]
    last = [x[rows - WINDOW_KEYS :] for x in (keys, values)]
    prior = lax.ppermute(
        jnp.concatenate(last, axis=1), "ep", [(i, i + 1) for i in range(lax.axis_size("ep") - 1)]
    )
    vmem = pl.BlockSpec(memory_space=pltpu.VMEM)
    smem = pl.BlockSpec(memory_space=pltpu.SMEM)
    return pl.pallas_call(
        attention_kernel,
        in_specs=[smem, smem] + [vmem] * 4,
        out_specs=vmem,
        out_shape=jax.ShapeDtypeStruct(queries.shape, jnp.bfloat16),
        compiler_params=params(12),
        cost_estimate=cost(10**9, 1 << 20),
        name="attention",
    )(lax.axis_index("ep").astype(jnp.int32).reshape(1), sinks, queries, keys, values, prior)


def combine_kernel(chunk_ref, target_ref, weight_ref, back_ref, before_ref, sum_ref, out_ref):
    tokens = target_ref.shape[0]
    rows = back_ref.shape[0]
    lane = lax.broadcasted_iota(jnp.int32, (tokens, rows), 1)
    place = lane % 8
    first = (lane // 8) * 16 + chunk_ref[0] * SLOTS

    def mixing(slot):
        mix = jnp.zeros((tokens, rows), jnp.float32)
        for k in range(TOPK):
            mix = jnp.where(target_ref[:, k : k + 1] == slot, weight_ref[:, k : k + 1], mix)
        main = mix.astype(jnp.bfloat16)
        return main, (mix - main.astype(jnp.float32)).astype(jnp.bfloat16)

    main = mixing(jnp.where(place < SLOTS, first + place, -1))
    last = jnp.zeros((tokens, LANES), jnp.float32)
    for b in range(BLOCKS + 1):
        cols = slice(b * LANES, (b + 1) * LANES)
        if b < BLOCKS:
            block = back_ref[:, cols]
            extra = mixing(jnp.where(place < SLOTS, -1, first + 2 * b + place - SLOTS))
            last = last + dot(extra[0], block) + dot(extra[1], block)
            value = dot(main[0], block) + dot(main[1], block)
        else:
            value = last
        value = value + before_ref[:, cols]
        sum_ref[:, cols] = value
        out_ref[:, cols] = value.astype(out_ref.dtype)


def combined(chunk, target, weight, back, before):
    vmem = pl.BlockSpec(memory_space=pltpu.VMEM)
    return pl.pallas_call(
        combine_kernel,
        in_specs=[pl.BlockSpec(memory_space=pltpu.SMEM)] + [vmem] * 4,
        out_specs=[vmem] * 2,
        out_shape=[
            jax.ShapeDtypeStruct(before.shape, jnp.float32),
            jax.ShapeDtypeStruct(before.shape, jnp.bfloat16),
        ],
        compiler_params=params(12),
        cost_estimate=cost(10**9, 2 << 20),
        name="combine",
    )(jnp.full((1,), chunk, jnp.int32), target, weight, back, before)


def program(
    projected_queries,
    key_proj,
    projected_values,
    head_sink_logits,
    out_weight,
    expert_input,
    norm_gain,
    routing,
    route_weight,
    gate_weight,
    up_weight,
    down_weight,
):
    bf = jnp.bfloat16
    tp = lax.axis_index("tp")
    at = tp.astype(jnp.int32).reshape(1)
    token_rows = expert_input.shape[0]
    experts = lax.axis_size("ep")
    share = D // N_TP

    ids = routing.T.reshape(-1)
    index = jnp.arange(ids.shape[0])
    same = (ids[:, None] == ids[None, :]) & (index[:, None] < index[None, :])
    rank = jnp.sum(same.astype(jnp.int32), axis=0)
    target = (ids * 16 + rank).reshape(TOPK, token_rows)

    gain = norm_gain[None, :]
    tp_index = tp.astype(jnp.int32)
    sent1 = dispatched(0, tp_index, target, expert_input, gain, experts * 8)
    got1 = exchanged(sent1)
    sent2 = dispatched(1, tp_index, target, expert_input, gain, experts * 8)
    got2 = exchanged(sent2)

    downs = []
    for k in range(N_TP):
        block = lax.dynamic_slice_in_dim(down_weight[0], ((tp + N_TP - k) % N_TP) * share, share, 1)
        downs.append(shifted(block, k) if k else block)

    def activated(got):
        middle = got.shape[0] // 2
        top, bottom = got[:middle], got[middle:]
        nt, pt = shifted(top, 1), shifted(top, -1)
        nb, pb = shifted(bottom, 1), shifted(bottom, -1)
        ft, fb = shifted(nt, 1), shifted(pb, -1)
        return hidden(at, got, (nt, nb, ft, fb, pt, pb), gate_weight[0], up_weight[0])

    def spread(act):
        return (act, shifted(act, 1), shifted(act, 2), shifted(act, -1))

    back1 = exchanged(results(spread(activated(got1)), downs))
    back2 = exchanged(results(spread(activated(got2)), downs))

    attended = attention(projected_queries, key_proj, projected_values, head_sink_logits)
    partial = dot(attended, out_weight).astype(bf)
    owned = partial.shape[0] // N_TP
    mixed = None
    for k in range(N_TP):
        block = lax.dynamic_slice_in_dim(partial, ((tp + N_TP - k) % N_TP) * owned, owned, 0)
        block = (shifted(block, k) if k else block).astype(jnp.float32)
        mixed = block if mixed is None else mixed + block
    mixer_output = mixed.astype(bf)

    columns = target.T
    start = jnp.zeros((token_rows, share), jnp.float32)
    so_far = combined(0, columns, route_weight, back1, start)[0]
    expert_output = combined(1, columns, route_weight, back2, so_far)[1]
    return (mixer_output, expert_output)


def solution(mesh):
    placed = (
        P("ep", "tp"),
        P("ep", "tp"),
        P("ep", "tp"),
        P("tp"),
        P("tp", None),
        P("ep", None),
        P(),
        P("ep", None),
        P("ep", None),
        P("ep", None, "tp"),
        P("ep", None, "tp"),
        P("ep", "tp", None),
    )
    return jax.shard_map(
        program,
        mesh=mesh,
        in_specs=placed,
        out_specs=(P(("ep", "tp"), None), P("ep", "tp")),
        check_vma=False,
    )
```

```python
import jax
import jax.numpy as jnp
from jax import lax
from jax.experimental import pallas as pl
from jax.experimental.pallas import tpu as pltpu
from jax.sharding import PartitionSpec as P

D = 4096
HEAD_SIZE = 64
WINDOW_KEYS = 128
TOPK = 4
EPS = 1e-06
CLAMP = 7.0
SLOPE = 1.702
N_TP = 4
SLOTS = 6
LANES = 256
BLOCKS = 3


def shifted(block, distance):
    return lax.ppermute(block, "tp", [((i + distance) % N_TP, i) for i in range(N_TP)])


def exchanged(block):
    return lax.all_to_all(block, "ep", split_axis=0, concat_axis=0, tiled=True)


def dot(a, b):
    return jnp.dot(a, b, preferred_element_type=jnp.float32)


def params(mib):
    return pltpu.CompilerParams(vmem_limit_bytes=mib << 20)


def cost(flops, size):
    return pl.CostEstimate(flops=flops, bytes_accessed=size, transcendentals=0)


def dispatch_kernel(chunk_ref, tp_ref, routing_ref, input_ref, gain_ref, out_ref, target_ref):
    rows = out_ref.shape[0]
    tokens, features = input_ref.shape
    share = features // N_TP
    own = pl.ds(pl.multiple_of(tp_ref[0] * share, share), share)
    squares = jnp.zeros((tokens, share), jnp.float32)
    for k in range(N_TP):
        part = input_ref[:, k * share : (k + 1) * share].astype(jnp.float32)
        squares = squares + part * part
    scale = lax.rsqrt(jnp.sum(squares, axis=1, keepdims=True) * (1.0 / features) + EPS)
    normed = (input_ref[:, own].astype(jnp.float32) * scale * gain_ref[:, own]).astype(jnp.bfloat16)

    experts = rows // 8
    expert = lax.broadcasted_iota(jnp.int32, (experts, tokens), 0)
    earlier = lax.broadcasted_iota(jnp.int32, (tokens, tokens), 0) < lax.broadcasted_iota(
        jnp.int32, (tokens, tokens), 1
    )
    earlier = jnp.where(earlier, 1.0, 0.0).astype(jnp.bfloat16)
    seen = jnp.zeros((experts, 1), jnp.float32)
    for k in range(TOPK):
        ids = routing_ref[k : k + 1, :]
        named = jnp.where(ids == expert, 1.0, 0.0)
        counts = dot(named.astype(jnp.bfloat16), earlier) + seen
        rank = jnp.sum(named * counts, axis=0, keepdims=True)
        target_ref[k : k + 1, :] = ids * 16 + rank.astype(jnp.int32)
        seen = seen + jnp.sum(named, axis=1, keepdims=True)
    row = lax.broadcasted_iota(jnp.int32, (rows, tokens), 0)
    place = row % 8
    first = (row // 8) * 16 + chunk_ref[0] * SLOTS

    def picks(slot):
        hit = target_ref[0:1, :] == slot
        for k in range(1, TOPK):
            hit = hit | (target_ref[k : k + 1, :] == slot)
        return jnp.where(hit, 1.0, 0.0).astype(jnp.bfloat16)

    main = picks(jnp.where(place < SLOTS, first + place, -1))
    last = normed[:, BLOCKS * LANES :]
    for b in range(BLOCKS):
        extra = picks(jnp.where(place < SLOTS, -1, first + 2 * b + place - SLOTS))
        cols = slice(b * LANES, (b + 1) * LANES)
        out_ref[:, cols] = (dot(main, normed[:, cols]) + dot(extra, last)).astype(out_ref.dtype)


def dispatched(chunk, tp, routing, tokens, gain, rows):
    vmem = pl.BlockSpec(memory_space=pltpu.VMEM)
    smem = pl.BlockSpec(memory_space=pltpu.SMEM)
    return pl.pallas_call(
        dispatch_kernel,
        in_specs=[smem, smem, vmem, vmem, vmem],
        out_specs=[vmem, vmem],
        out_shape=[
            jax.ShapeDtypeStruct((rows, BLOCKS * LANES), jnp.bfloat16),
            jax.ShapeDtypeStruct(routing.shape, jnp.int32),
        ],
        compiler_params=params(56),
        cost_estimate=cost(4 * rows * 128 * 768, 1 << 20),
        name="dispatch",
    )(jnp.full((1,), chunk, jnp.int32), tp, routing, tokens, gain)


def hidden_kernel(
    tp_ref, own, nt, nb, ft, fb, pt, pb, gate_ref, up_ref, out_ref, held, weights, acc, sems
):
    step = pl.program_id(0)
    rows = own.shape[0]
    width = BLOCKS * LANES
    half = rows // 2
    depth = weights.shape[2]
    loads = []
    for j, pieces in enumerate(((own,), (nt, nb), (ft, fb), (pt, pb))):
        at = pl.ds(((tp_ref[0] + j) % N_TP) * depth, depth)
        these = [
            pltpu.make_async_copy(gate_ref.at[at], weights.at[j, 0], sems.at[j, 0]),
            pltpu.make_async_copy(up_ref.at[at], weights.at[j, 1], sems.at[j, 1]),
        ]
        for k, piece in enumerate(pieces):
            place = held.at[j] if j == 0 else held.at[j, pl.ds(k * half, half)]
            these.append(pltpu.make_async_copy(piece, place, sems.at[j, 2 + k]))
        loads.append(these)

    @pl.when(step == 0)
    def _():
        for these in loads:
            for load in these:
                load.start()

    for j, these in enumerate(loads):

        @pl.when(step == j)
        def _():
            for load in these:
                load.wait()

    shape = (rows // 8, 8, LANES)
    place = lax.broadcasted_iota(jnp.int32, shape, 1)
    moved = [
        pltpu.roll(
            held[step, :, b * LANES : (b + 1) * LANES].astype(jnp.float32).reshape(shape), 2 * b + 2, 1
        )
        for b in range(BLOCKS)
    ]
    last = jnp.where(place < 2, moved[0], jnp.where(place < 4, moved[1], moved[2]))
    last = last.reshape(rows, LANES).astype(jnp.bfloat16)
    for side in range(2):
        term = dot(held[step], weights[step, side, :width, :]) + dot(
            last, weights[step, side, width:, :]
        )
        acc[side] = jnp.where(step == 0, term, acc[side] + term)

    @pl.when(step == N_TP - 1)
    def _():
        gate_cut = jnp.minimum(acc[0], CLAMP)
        up_cut = jnp.clip(acc[1], -CLAMP, CLAMP)
        value = ((up_cut + 1.0) * gate_cut * jax.nn.sigmoid(SLOPE * gate_cut)).reshape(shape)
        count = rows // 32
        low = place[:count] < SLOTS
        fourth = value[BLOCKS * count :]
        for b in range(BLOCKS):
            packed = jnp.where(
                low, value[b * count : (b + 1) * count], pltpu.roll(fourth, SLOTS - 2 * b, 1)
            )
            out_ref[b * count * 8 : (b + 1) * count * 8, :] = packed.reshape(count * 8, LANES).astype(
                out_ref.dtype
            )


def hidden(tp, own, pieces, gate, up):
    rows, width = own.shape
    cols = gate.shape[1]
    return pl.pallas_call(
        hidden_kernel,
        grid_spec=pltpu.PrefetchScalarGridSpec(
            num_scalar_prefetch=1,
            grid=(N_TP,),
            in_specs=[pl.BlockSpec(memory_space=pl.ANY)] * 9,
            out_specs=pl.BlockSpec((rows * 3 // 4, cols), lambda j, t: (0, 0)),
            scratch_shapes=[
                pltpu.VMEM((N_TP, rows, width), jnp.bfloat16),
                pltpu.VMEM((N_TP, 2, width + LANES, cols), jnp.bfloat16),
                pltpu.VMEM((2, rows, cols), jnp.float32),
                pltpu.SemaphoreType.DMA((N_TP, 4)),
            ],
        ),
        out_shape=jax.ShapeDtypeStruct((rows * 3 // 4, cols), jnp.bfloat16),
        compiler_params=params(56),
        cost_estimate=cost(8 * rows * width * cols, 8 << 20),
        name="hidden",
    )(tp, own, *pieces, gate, up)


def result_kernel(a0, a1, a2, a3, d0, d1, d2, d3, out_ref):
    res = dot(a0[...], d0[...])
    for a, d in ((a1, d1), (a2, d2), (a3, d3)):
        res = res + dot(a[...], d[...])
    count = res.shape[0] // 24
    shape = (BLOCKS * count, 8, LANES)
    place = lax.broadcasted_iota(jnp.int32, (count, 8, LANES), 1)

    def unpacked(cols):
        value = res[:, cols].reshape(shape)
        parts = [value[b * count : (b + 1) * count] for b in range(BLOCKS)]
        moved = [pltpu.roll(part, 2 * b + 2, 1) for b, part in enumerate(parts)]
        return parts + [jnp.where(place < 2, moved[0], jnp.where(place < 4, moved[1], moved[2]))]

    last = unpacked(slice(BLOCKS * LANES, (BLOCKS + 1) * LANES))
    for b in range(BLOCKS):
        main = unpacked(slice(b * LANES, (b + 1) * LANES))
        for q in range(4):
            block = jnp.where(place < SLOTS, main[q], pltpu.roll(last[q], SLOTS - 2 * b, 1))
            out_ref[q * count * 8 : (q + 1) * count * 8, b * LANES : (b + 1) * LANES] = block.reshape(
                count * 8, LANES
            ).astype(out_ref.dtype)


def results(acts, downs):
    rows = acts[0].shape[0]
    return pl.pallas_call(
        result_kernel,
        out_shape=jax.ShapeDtypeStruct((rows * 4 // 3, BLOCKS * LANES), jnp.bfloat16),
        compiler_params=params(14),
        cost_estimate=cost(2 * rows * 1024 * 1024, 4 << 20),
        name="results",
    )(*acts, *downs)


def attention_kernel(ep_ref, sink_ref, q_ref, k_ref, v_ref, prior_ref, out_ref):
    block = WINDOW_KEYS
    tiles = q_ref.shape[1] // 128
    query = lax.broadcasted_iota(jnp.int32, (block, 2 * block), 0)
    key = lax.broadcasted_iota(jnp.int32, (block, 2 * block), 1)
    lane = lax.broadcasted_iota(jnp.int32, (block, 128), 1)
    for n in range(q_ref.shape[0] // block):
        own = slice(n * block, (n + 1) * block)
        before = slice((n - 1) * block, n * block)
        allowed = (key > query) & (key <= query + block)
        if n == 0:
            allowed = allowed & (key >= jnp.where(ep_ref[0] == 0, block, 0))
            key_prior, value_prior = prior_ref[:, :128], prior_ref[:, 128:]
        else:
            key_prior, value_prior = k_ref[before, :], v_ref[before, :]
        keys = jnp.concatenate([key_prior, k_ref[own, :]], axis=0)
        values = jnp.concatenate([value_prior, v_ref[own, :]], axis=0)
        for t in range(tiles):
            tile = q_ref[own, t * 128 : (t + 1) * 128].astype(jnp.float32)
            group = t // 2
            parts = []
            for e in range(2):
                head = tile if e == group else pltpu.roll(tile, HEAD_SIZE, 1)
                head = jnp.where(lane // HEAD_SIZE == group, head, 0.0).astype(jnp.bfloat16)
                scores = lax.dot_general(
                    head, keys, (((1,), (1,)), ((), ())), preferred_element_type=jnp.float32
                ) * HEAD_SIZE ** (-0.5)
                scores = jnp.where(allowed, scores, -jnp.inf)
                sink = sink_ref[2 * t + e]
                highest = jnp.maximum(jnp.max(scores, axis=1, keepdims=True), sink)
                numerator = jnp.exp(scores - highest)
                denominator = jnp.sum(numerator, axis=1, keepdims=True) + jnp.exp(sink - highest)
                weights = (numerator * (1.0 / denominator)).astype(jnp.bfloat16)
                result = dot(weights, values)
                parts.append(result if e == group else pltpu.roll(result, HEAD_SIZE, 1))
            out_ref[own, t * 128 : (t + 1) * 128] = jnp.where(
                lane < HEAD_SIZE, parts[0], parts[1]
            ).astype(out_ref.dtype)


def attention(queries, keys, values, sinks):
    rows = queries.shape[0]
    last = [x[rows - WINDOW_KEYS :] for x in (keys, values)]
    prior = lax.ppermute(
        jnp.concatenate(last, axis=1), "ep", [(i, i + 1) for i in range(lax.axis_size("ep") - 1)]
    )
    vmem = pl.BlockSpec(memory_space=pltpu.VMEM)
    smem = pl.BlockSpec(memory_space=pltpu.SMEM)
    return pl.pallas_call(
        attention_kernel,
        in_specs=[smem, smem] + [vmem] * 4,
        out_specs=vmem,
        out_shape=jax.ShapeDtypeStruct(queries.shape, jnp.bfloat16),
        compiler_params=params(12),
        cost_estimate=cost(10**9, 1 << 20),
        name="attention",
    )(lax.axis_index("ep").astype(jnp.int32).reshape(1), sinks, queries, keys, values, prior)


def combine_kernel(chunk_ref, target_ref, weight_ref, back_ref, before_ref, sum_ref, out_ref):
    tokens = target_ref.shape[0]
    rows = back_ref.shape[0]
    lane = lax.broadcasted_iota(jnp.int32, (tokens, rows), 1)
    place = lane % 8
    first = (lane // 8) * 16 + chunk_ref[0] * SLOTS

    def mixing(slot):
        mix = jnp.zeros((tokens, rows), jnp.float32)
        for k in range(TOPK):
            mix = jnp.where(target_ref[:, k : k + 1] == slot, weight_ref[:, k : k + 1], mix)
        main = mix.astype(jnp.bfloat16)
        return main, (mix - main.astype(jnp.float32)).astype(jnp.bfloat16)

    main = mixing(jnp.where(place < SLOTS, first + place, -1))
    last = jnp.zeros((tokens, LANES), jnp.float32)
    for b in range(BLOCKS + 1):
        cols = slice(b * LANES, (b + 1) * LANES)
        if b < BLOCKS:
            block = back_ref[:, cols]
            extra = mixing(jnp.where(place < SLOTS, -1, first + 2 * b + place - SLOTS))
            last = last + dot(extra[0], block) + dot(extra[1], block)
            value = dot(main[0], block) + dot(main[1], block)
        else:
            value = last
        value = value + before_ref[:, cols]
        sum_ref[:, cols] = value
        out_ref[:, cols] = value.astype(out_ref.dtype)


def combined(chunk, target, weight, back, before):
    vmem = pl.BlockSpec(memory_space=pltpu.VMEM)
    return pl.pallas_call(
        combine_kernel,
        in_specs=[pl.BlockSpec(memory_space=pltpu.SMEM)] + [vmem] * 4,
        out_specs=[vmem] * 2,
        out_shape=[
            jax.ShapeDtypeStruct(before.shape, jnp.float32),
            jax.ShapeDtypeStruct(before.shape, jnp.bfloat16),
        ],
        compiler_params=params(12),
        cost_estimate=cost(10**9, 2 << 20),
        name="combine",
    )(jnp.full((1,), chunk, jnp.int32), target, weight, back, before)


def program(
    projected_queries,
    key_proj,
    projected_values,
    head_sink_logits,
    out_weight,
    expert_input,
    norm_gain,
    routing,
    route_weight,
    gate_weight,
    up_weight,
    down_weight,
):
    bf = jnp.bfloat16
    tp = lax.axis_index("tp")
    at = tp.astype(jnp.int32).reshape(1)
    token_rows = expert_input.shape[0]
    experts = lax.axis_size("ep")
    share = D // N_TP

    gain = norm_gain[None, :]
    named = routing.T
    sent1, target = dispatched(0, at, named, expert_input, gain, experts * 8)
    got1 = exchanged(sent1)
    got2 = exchanged(dispatched(1, at, named, expert_input, gain, experts * 8)[0])

    downs = []
    for k in range(N_TP):
        block = lax.dynamic_slice_in_dim(down_weight[0], ((tp + N_TP - k) % N_TP) * share, share, 1)
        downs.append(shifted(block, k) if k else block)

    def activated(got):
        middle = got.shape[0] // 2
        top, bottom = got[:middle], got[middle:]
        nt, pt = shifted(top, 1), shifted(top, -1)
        nb, pb = shifted(bottom, 1), shifted(bottom, -1)
        ft, fb = shifted(nt, 1), shifted(pb, -1)
        return hidden(at, got, (nt, nb, ft, fb, pt, pb), gate_weight[0], up_weight[0])

    def spread(act):
        return (act, shifted(act, 1), shifted(act, 2), shifted(act, -1))

    back1 = exchanged(results(spread(activated(got1)), downs))
    back2 = exchanged(results(spread(activated(got2)), downs))

    attended = attention(projected_queries, key_proj, projected_values, head_sink_logits)
    partial = dot(attended, out_weight).astype(bf)
    owned = partial.shape[0] // N_TP
    mixed = None
    for k in range(N_TP):
        block = lax.dynamic_slice_in_dim(partial, ((tp + N_TP - k) % N_TP) * owned, owned, 0)
        block = (shifted(block, k) if k else block).astype(jnp.float32)
        mixed = block if mixed is None else mixed + block
    mixer_output = mixed.astype(bf)

    columns = target.T
    start = jnp.zeros((token_rows, share), jnp.float32)
    so_far = combined(0, columns, route_weight, back1, start)[0]
    expert_output = combined(1, columns, route_weight, back2, so_far)[1]
    return (mixer_output, expert_output)


def solution(mesh):
    placed = (
        P("ep", "tp"),
        P("ep", "tp"),
        P("ep", "tp"),
        P("tp"),
        P("tp", None),
        P("ep", None),
        P(),
        P("ep", None),
        P("ep", None),
        P("ep", None, "tp"),
        P("ep", None, "tp"),
        P("ep", "tp", None),
    )
    return jax.shard_map(
        program,
        mesh=mesh,
        in_specs=placed,
        out_specs=(P(("ep", "tp"), None), P("ep", "tp")),
        check_vma=False,
    )
```
